32 devices in a mesh: fs: 8 (over z, x), tp: 4 (over y, core).
Axes of the slice: x: 2, y: 2, z: 4, core: 2. Of those that a mesh axis runs over, the one named last changes fastest.
Arguments:
- tokens: bfloat16 [4096, 2048], P(('fs', 'tp')), may hold values from -6 to 6
- norm_gain: float32 [2048], P('fs'), may hold values from 0.1 to 1.9
- gate_proj: float32 [32, 2048, 512], P(None, 'fs', 'tp'), may hold values from -0.125 to 0.125
- up_proj: float32 [32, 2048, 512], P(None, 'fs', 'tp'), may hold values from -0.125 to 0.125
- down_proj: float32 [32, 512, 2048], P(None, 'fs', 'tp'), may hold values from -0.25 to 0.25
- expert_ids: int32 [4096, 2], P(('fs', 'tp')), may hold values from 0 to 31, as said below
- route_weight: float32 [4096, 2], P(('fs', 'tp')), may hold values from 0.05 to 1
Outputs:
- mixed: bfloat16 [4096, 2048], P(('fs', 'tp'))
- new_gate: bfloat16 [32, 2048, 512], P(('fs', 'tp'))
- new_up: bfloat16 [32, 2048, 512], P(('fs', 'tp'))
- new_down: bfloat16 [32, 512, 2048], P(('fs', 'tp'))
The draws below stay inside these ranges and needn't reach their ends.
Inputs may be any that keep to these rules, and one draw needn't show every extreme that they name: `expert_ids`: the two experts of a row differ and lie in one group of 4 consecutive experts. In each aligned block of 128 rows (the rows of one device) every group is named by exactly 16 rows, no expert by more than 16 rows, and one expert, the same in all blocks, by exactly 16 rows.
All inputs are finite; a program needn't handle non-finite values.
Results may differ from the reference program's by a relative error of at most 0.0087.
Values may be sent and summed in bfloat16 or wider, within the bound.
No kernel may reach another device: no remote copies, remote signals or barrier semaphores. Data moves between devices by JAX's collectives and lax.ppermute only.
A program may use at most 128 MiB of HBM per device.

```python
import jax
import jax.numpy as jnp
from jax import lax

D = 2048
FF = 512
EPG = 4
TOK_DEV = 128
EXPERTS = 32
GROUPS = 8
CAP = 16
TOKENS = 4096


def draw_expert_ids(key, part):
    key_hot, key_blocks = jax.random.split(jax.random.fold_in(key, 17))
    hot_expert = jax.random.randint(key_hot, (), 0, EXPERTS)
    hot_group = hot_expert // EPG
    hot_slot = hot_expert % EPG

    def draw_block(block_key):
        key_order, key_first, key_second = jax.random.split(block_key, 3)
        position = jax.random.permutation(key_order, TOK_DEV)
        group_index = (hot_group + position // CAP) % GROUPS
        first_pick = jax.random.randint(key_first, (TOK_DEV,), 0, EPG)
        first_pick = jnp.where(position < CAP, hot_slot, first_pick)
        second_pick = (first_pick + jax.random.randint(key_second, (TOK_DEV,), 1, EPG)) % EPG
        return jnp.stack([group_index * EPG + first_pick, group_index * EPG + second_pick], axis=-1)
    block_keys = jax.random.split(key_blocks, TOKENS // TOK_DEV)
    return jax.vmap(draw_block)(block_keys).reshape(TOKENS, 2).astype(jnp.int32)


def shard_levels(key, dims, cuts, low, largest):
    def one(axis_at, parts):
        heights = jax.random.uniform(jax.random.fold_in(jax.random.fold_in(key, 6), axis_at), (parts,), jnp.float32, low / len(cuts), largest / len(cuts))
        return jnp.repeat(jnp.exp(heights), dims[axis_at] // parts).reshape((-1,) + (1,) * (len(dims) - axis_at - 1))

    gain = one(*cuts[0])
    for cut in cuts[1:]:
        gain = gain * one(*cut)
    return gain


def normal_values(key, shape, spread, most, cuts=(), held_as=jnp.bfloat16):
    array = jax.random.normal(key, shape, jnp.float32) * spread
    if len(cuts) > 0:
        array = shard_levels(key, shape, cuts, -0.22, 0.18) * array
    return jnp.clip(array, min=-most, max=most).astype(held_as)


def setup_inputs(seed: int = 0) -> dict:
    arg_keys = jax.random.split(jax.random.key(seed), 8)
    return {
        "tokens": normal_values(arg_keys[0], (TOKENS, D), 1.0, 6.0, ((0, 32),)),
        "norm_gain": jnp.clip(1.0 + 0.18 * jax.random.normal(arg_keys[1], (D,), jnp.float32), 0.1, 1.9),
        "gate_proj": normal_values(arg_keys[2], (EXPERTS, D, FF), D ** -0.5, 0.125, ((1, 8), (2, 4)), jnp.float32),
        "up_proj": normal_values(arg_keys[3], (EXPERTS, D, FF), D ** -0.5, 0.125, ((1, 8), (2, 4)), jnp.float32),
        "down_proj": normal_values(arg_keys[4], (EXPERTS, FF, D), FF ** -0.5, 0.25, ((1, 8), (2, 4)), jnp.float32),
        "expert_ids": draw_expert_ids(jax.random.fold_in(arg_keys[7], 71), 0),
        "route_weight": jnp.clip(0.05 + 0.95 * jax.random.uniform(arg_keys[6], (TOKENS, 2), jnp.float32) ** shard_levels(arg_keys[6], (TOKENS, 2), ((0, 32),), -0.2, 0.2), 0.05, 1.0),
    }


norm_eps = 1e-06

def reference(tokens, norm_gain, gate_proj, up_proj, down_proj, expert_ids, route_weight):
    row_scale = norm_gain[None, :, None]
    new_gate = (gate_proj * row_scale).astype(jnp.bfloat16)
    new_up = (up_proj * row_scale).astype(jnp.bfloat16)
    new_down = down_proj.astype(jnp.bfloat16)
    widened = tokens.astype(jnp.float32)
    normed = (widened * lax.rsqrt(lax.optimization_barrier(jnp.mean(widened * widened, axis=-1, keepdims=True)) + norm_eps)).astype(jnp.bfloat16)
    flat_ids = expert_ids.reshape(-1)
    flat_weight = route_weight.reshape(-1)
    most_rows = CAP * (TOKENS // TOK_DEV)

    def add_expert(expert, mixed_sum):
        named = flat_ids == expert
        pick_index = jnp.nonzero(named, size=most_rows, fill_value=0)[0]
        pick_count = jnp.sum(named.astype(jnp.int32))
        live_pick = jnp.arange(most_rows, dtype=jnp.int32) < pick_count
        token_rows = normed[pick_index // 2]
        gate_act = jnp.dot(token_rows, new_gate[expert], preferred_element_type=jnp.float32)
        up_act = jnp.dot(token_rows, new_up[expert], preferred_element_type=jnp.float32)
        hidden = (jax.nn.silu(gate_act) * up_act).astype(jnp.bfloat16)
        expert_out = jnp.dot(hidden, new_down[expert], preferred_element_type=jnp.float32).astype(jnp.bfloat16)
        weights = jnp.where(live_pick, flat_weight[pick_index], jnp.zeros((), jnp.float32))
        return mixed_sum.at[pick_index // 2].add(weights[:, None] * expert_out.astype(jnp.float32))
    mixed_sum = lax.fori_loop(0, EXPERTS, add_expert, jnp.zeros((TOKENS, D), jnp.float32))
    return (mixed_sum.astype(jnp.bfloat16), new_gate, new_up, new_down)
```

```python
import functools

import jax
import jax.numpy as jnp
from jax import lax
from jax.experimental import pallas as pl
from jax.experimental.pallas import tpu as pltpu
from jax.sharding import PartitionSpec as P

norm_eps = 1e-06
lanes = 128
bf16 = jnp.bfloat16
f32 = jnp.float32


def cost(flops, nbytes):
    return pl.CostEstimate(flops=int(flops), bytes_accessed=int(nbytes), transcendentals=0)


def slot_onehot(group_col, group_row, per_group):
    count = group_col.shape[0]
    row = lax.broadcasted_iota(jnp.int32, (count, count), 0)
    col = lax.broadcasted_iota(jnp.int32, (count, count), 1)
    earlier = jnp.where((group_col == group_row) & (col < row), 1.0, 0.0)
    rank = jnp.sum(earlier, axis=1, keepdims=True).astype(jnp.int32)
    slot = group_col * per_group + rank
    return jnp.where(slot == col, 1.0, 0.0).astype(bf16)


def prep_kernel(per_group, tp, tok_ref, gcol_ref, grow_ref, local_ref, weight_ref, out_ref):
    count, width = tok_ref.shape
    onehot = slot_onehot(gcol_ref[...], grow_ref[...], per_group)
    wide = tok_ref[...].astype(f32)
    scale = lax.rsqrt(jnp.mean(wide * wide, axis=-1, keepdims=True) + norm_eps)
    normed = (wide * scale).astype(bf16)
    lane = lax.broadcasted_iota(jnp.int32, (count, lanes), 1)
    extra = jnp.zeros((count, lanes), f32)
    for pick in range(2):
        local = local_ref[:, pick : pick + 1]
        rest = weight_ref[:, pick : pick + 1]
        for part in range(3):
            piece = rest.astype(bf16).astype(f32)
            extra = extra + jnp.where(lane == local + part * tp, piece, 0.0)
            rest = rest - piece
    dims = (((0,), (0,)), ((), ()))
    out_ref[:, :width] = lax.dot_general(onehot, normed, dims, preferred_element_type=f32).astype(bf16)
    out_ref[:, width:] = lax.dot_general(
        onehot, extra.astype(bf16), dims, preferred_element_type=f32
    ).astype(bf16)


def regroup_kernel(fs, *refs):
    out_ref = refs[fs]
    for r in range(fs):
        out_ref[0, r] = refs[r][0]


def regroup(parts):
    fs = len(parts)
    tp, rows, cols = parts[0].shape
    return pl.pallas_call(
        functools.partial(regroup_kernel, fs),
        grid=(tp,),
        in_specs=[pl.BlockSpec((1, rows, cols), lambda e: (e, 0, 0))] * fs,
        out_specs=pl.BlockSpec((1, fs, rows, cols), lambda e: (e, 0, 0, 0)),
        out_shape=jax.ShapeDtypeStruct((tp, fs, rows, cols), bf16),
        cost_estimate=cost(1e9, 4 * fs * tp * rows * cols),
        name="regroup",
    )(*parts)


def project_kernel(fs, tp, last, me_ref, pieces_ref, *refs):
    x_refs, refs = refs[:tp], refs[tp:]
    if last:
        gate_ref, matrix_ref, out_ref, total = refs
    else:
        matrix_ref, total = refs
    step = pl.program_id(0)
    block = jnp.concatenate([pieces_ref[j, 0] for j in range(tp)], axis=-1)
    matrix_ref[...] = block
    rows = jnp.concatenate([ref[...] for ref in x_refs], axis=0)
    product = jnp.dot(rows, block, preferred_element_type=f32)

    @pl.when(step == 0)
    def _():
        total[...] = product

    @pl.when(step > 0)
    def _():
        total[...] += product

    if last:

        @pl.when(step == fs - 1)
        def _():
            gate = gate_ref[...]
            out_ref[...] = (gate / (1.0 + jnp.exp(-gate)) * total[...]).astype(bf16)


def project(me, pieces, rows, gate=None):
    tp, fs, height, cols = pieces.shape
    count = rows[0].shape[0]
    last = gate is not None

    def origin(r, me_ref):
        return lax.rem(me_ref[0] - r + fs, fs)

    in_specs = [pl.BlockSpec((tp, 1, height, cols), lambda r, m: (0, r, 0, 0))]
    in_specs += [pl.BlockSpec((count, height), lambda r, m: (0, origin(r, m)))] * tp
    args = [pieces, *rows]
    whole = pl.BlockSpec((tp * count, tp * cols), lambda r, m: (0, 0))
    out_specs = [pl.BlockSpec((height, tp * cols), lambda r, m: (origin(r, m), 0))]
    out_shape = [jax.ShapeDtypeStruct((fs * height, tp * cols), bf16)]
    scratch = []
    if last:
        in_specs.append(whole)
        args.append(gate)
        out_shape.append(jax.ShapeDtypeStruct((tp * count, tp * cols), bf16))
        scratch = [pltpu.VMEM((tp * count, tp * cols), f32)]
    else:
        out_shape.append(jax.ShapeDtypeStruct((tp * count, tp * cols), f32))
    out_specs.append(whole)
    flops = 2 * tp * count * fs * height * tp * cols
    return pl.pallas_call(
        functools.partial(project_kernel, fs, tp, last),
        grid_spec=pltpu.PrefetchScalarGridSpec(
            num_scalar_prefetch=1,
            grid=(fs,),
            in_specs=in_specs,
            out_specs=out_specs,
            scratch_shapes=scratch,
        ),
        out_shape=out_shape,
        cost_estimate=cost(flops, 8 * fs * height * tp * cols),
        name="up_rows" if last else "gate_rows",
    )(me, *args)


def split_kernel(fs, tp, bounds, me_ref, in_ref, *out_refs):
    for r in range(fs):
        target = lax.rem(me_ref[0] + r, fs)
        full = jnp.concatenate([in_ref[j, target] for j in range(tp)], axis=-1)
        for h, (low, high) in enumerate(bounds):
            out_refs[h * fs + r][...] = full[:, low:high]


def split_down(me, arrived, bounds):
    tp, fs, rows, cols = arrived.shape
    shapes = [
        jax.ShapeDtypeStruct((rows, high - low), bf16) for low, high in bounds for _ in range(fs)
    ]
    outs = pl.pallas_call(
        functools.partial(split_kernel, fs, tp, bounds),
        in_specs=[pl.BlockSpec(memory_space=pltpu.SMEM), pl.BlockSpec(memory_space=pltpu.VMEM)],
        out_specs=[pl.BlockSpec(memory_space=pltpu.VMEM)] * len(shapes),
        out_shape=shapes,
        cost_estimate=cost(1e9, 4 * tp * fs * rows * cols),
        name="split_down",
    )(me, arrived)
    return [outs[h * fs : (h + 1) * fs] for h in range(len(bounds))]


def down_kernel(fs, tp, direct, aliased, me_ref, hidden_ref, *refs):
    w_refs, refs = refs[:tp], refs[tp:]
    parts, refs = refs[:fs], refs[fs:]
    if aliased:
        refs = refs[1:]
    matrix_ref, out_ref, block = refs
    rows = parts[0].shape[0]
    for r in range(fs):
        origin = lax.rem(me_ref[0] - r + fs, fs)
        block[pl.ds(pl.multiple_of(origin * rows, rows), rows), :] = parts[r][...]
    matrix_ref[...] = block[...]
    product = jnp.dot(hidden_ref[...], block[...], preferred_element_type=f32)
    product = product.astype(bf16).astype(f32)
    count = w_refs[0].shape[0]
    lane = lax.broadcasted_iota(jnp.int32, (count, lanes), 1)
    mine = me_ref[1]
    chosen = (lane == mine) | (lane == mine + tp) | (lane == mine + 2 * tp)
    for q in range(tp):
        weight = jnp.sum(
            jnp.where(chosen, w_refs[q][...].astype(f32), 0.0), axis=1, keepdims=True
        )
        scaled = (product[q * count : (q + 1) * count] * weight).astype(bf16)
        source = lax.rem(mine - q + tp, tp)
        if direct:
            each = count // fs
            for i in range(fs):
                out_ref[i, source] = scaled[i * each : (i + 1) * each]
        else:
            out_ref[source] = scaled


def down_rows(me, hidden, rows, parts, bound, width, prior, direct):
    tp, fs = len(rows), len(parts)
    count = rows[0].shape[0]
    depth = hidden.shape[1]
    low, high = bound
    size = high - low
    col_block = low // size
    weight_block = width // lanes
    in_specs = [pl.BlockSpec(hidden.shape, lambda k, m: (0, 0))]
    in_specs += [pl.BlockSpec((count, lanes), lambda k, m: (0, weight_block))] * tp
    in_specs += [pl.BlockSpec(parts[0].shape, lambda k, m: (0, 0))] * fs
    args = [hidden, *rows, *parts]
    aliases = {}
    if prior is not None:
        in_specs.append(pl.BlockSpec(memory_space=pl.ANY))
        args.append(prior)
        aliases = {len(args): 0}
    shape = (fs, tp, count // fs, size) if direct else (tp, count, size)
    return pl.pallas_call(
        functools.partial(down_kernel, fs, tp, direct, prior is not None),
        grid_spec=pltpu.PrefetchScalarGridSpec(
            num_scalar_prefetch=1,
            grid=(1,),
            in_specs=in_specs,
            out_specs=[
                pl.BlockSpec((depth, size), lambda k, m: (0, col_block)),
                pl.BlockSpec(shape, lambda k, m: (0,) * len(shape)),
            ],
            scratch_shapes=[pltpu.VMEM((depth, size), bf16)],
        ),
        out_shape=[
            jax.ShapeDtypeStruct((depth, width), bf16),
            jax.ShapeDtypeStruct(shape, bf16),
        ],
        input_output_aliases=aliases,
        cost_estimate=cost(2 * tp * count * depth * size, 4 * depth * size),
        name="down_rows",
    )(me, *args)


def final_kernel(per_group, bounds, gcol_ref, grow_ref, *refs):
    out_ref = refs[-1]
    onehot = slot_onehot(gcol_ref[...], grow_ref[...], per_group)
    for (low, high), ref in zip(bounds, refs[:-1]):
        if len(ref.shape) == 4:
            groups, tp, each, _ = ref.shape
            back = jnp.concatenate(
                [
                    functools.reduce(
                        lambda a, b: a + b, [ref[g, e].astype(f32) for e in range(tp)]
                    ).astype(bf16)
                    for g in range(groups)
                ],
                axis=0,
            )
        else:
            back = ref[...]
        out_ref[:, low:high] = jnp.dot(onehot, back, preferred_element_type=f32).astype(bf16)


def pieces_of(width):
    half, quarter = width // 2, width // 4
    return [(0, half, False), (half, half + quarter, False), (half + quarter, width, False)]


def shards(tokens, norm_gain, gate_proj, up_proj, down_proj, expert_ids, route_weight):
    fs = lax.axis_size("fs")
    tp = lax.axis_size("tp")
    fi = lax.axis_index("fs")
    ti = lax.axis_index("tp")
    me = jnp.stack([fi, ti]).astype(jnp.int32)
    count, width = tokens.shape
    per_group = count // fs
    plan = pieces_of(width)
    bounds = [(low, high) for low, high, _ in plan]

    def shift(axis, n, step):
        return [(k, (k + step) % n) for k in range(n)]

    def spread(parts):
        return [parts[0]] + [
            lax.ppermute(parts[r], "fs", shift("fs", fs, r)) for r in range(1, fs)
        ]

    def cut(matrix, scale):
        out = []
        for r in range(fs):
            start = lax.rem(fi + r, fs) * tp
            piece = lax.dynamic_slice(
                matrix, (start, 0, 0), (tp,) + matrix.shape[1:]
            )
            out.append((piece * scale).astype(bf16))
        return out

    scale = norm_gain[None, :, None]

    group = expert_ids[:, :1] // tp
    group_row = group.reshape(1, count)
    local = expert_ids - group * tp
    sorted_rows = pl.pallas_call(
        functools.partial(prep_kernel, per_group, tp),
        out_shape=jax.ShapeDtypeStruct((count, width + lanes), bf16),
        cost_estimate=cost(2 * count * count * width, 4 * count * width),
        name="prep_rows",
    )(tokens, group, group_row, local, route_weight)

    gate_parts = spread(cut(gate_proj, scale))
    sent = sorted_rows.reshape(fs, per_group, width + lanes)
    landed = lax.all_to_all(sent, "fs", 0, 0, tiled=True).reshape(count, width + lanes)
    rows = [landed] + [
        lax.ppermute(landed, "tp", shift("tp", tp, q)) for q in range(1, tp)
    ]

    down_low = down_proj.reshape((fs, tp) + down_proj.shape[1:]).astype(bf16).transpose(1, 0, 2, 3)
    down_here = lax.all_to_all(down_low, "tp", 0, 0, tiled=True)
    up_parts = spread(cut(up_proj, scale))
    down_parts = [spread(list(parts)) for parts in split_down(me, down_here, bounds)]

    gate_pieces = lax.all_to_all(regroup(gate_parts), "tp", 0, 0, tiled=True)
    new_gate, gate_act = project(me, gate_pieces, rows)
    up_pieces = lax.all_to_all(regroup(up_parts), "tp", 0, 0, tiled=True)
    new_up, hidden = project(me, up_pieces, rows, gate_act)

    new_down = None
    backs = []
    for parts, (low, high, direct) in zip(down_parts, plan):
        new_down, partial = down_rows(
            me, hidden, rows, parts, (low, high), width, new_down, direct
        )
        if direct:
            back = lax.all_to_all(
                partial.reshape(fs * tp, per_group, high - low), ("fs", "tp"), 0, 0, tiled=True
            ).reshape(partial.shape)
        else:
            shared = lax.all_to_all(partial, "tp", 0, 0, tiled=True)
            summed = jnp.sum(shared.astype(f32), axis=0).astype(bf16)
            back = lax.all_to_all(
                summed.reshape(fs, per_group, high - low), "fs", 0, 0, tiled=True
            ).reshape(count, high - low)
        backs.append(back)
    mixed = pl.pallas_call(
        functools.partial(final_kernel, per_group, bounds),
        out_shape=jax.ShapeDtypeStruct((count, width), bf16),
        cost_estimate=cost(2 * count * count * width, 4 * count * width),
        name="final_rows",
    )(group, group_row, *backs)
    return (mixed, new_gate[None], new_up[None], new_down[None])


def solution(mesh):
    in_specs = (
        P(("fs", "tp"), None),
        P("fs"),
        P(None, "fs", "tp"),
        P(None, "fs", "tp"),
        P(None, "fs", "tp"),
        P(("fs", "tp"), None),
        P(("fs", "tp"), None),
    )
    out_specs = (
        P(("fs", "tp"), None),
        P(("fs", "tp"), None, None),
        P(("fs", "tp"), None, None),
        P(("fs", "tp"), None, None),
    )
    return jax.shard_map(shards, mesh=mesh, in_specs=in_specs, out_specs=out_specs, check_vma=False)
```

```python
import functools

import jax
import jax.numpy as jnp
from jax import lax
from jax.experimental import pallas as pl
from jax.experimental.pallas import tpu as pltpu
from jax.sharding import PartitionSpec as P


norm_eps = 1e-06
lanes = 128
bf16 = jnp.bfloat16
f32 = jnp.float32
grant = 24 * 1024 * 1024


def cost(flops, nbytes):
    return pl.CostEstimate(flops=int(flops), bytes_accessed=int(nbytes), transcendentals=0)


def params():
    return pltpu.CompilerParams(vmem_limit_bytes=grant)


def whole(shape):
    return pl.BlockSpec(shape, lambda *_: (0,) * len(shape))


def square(n):
    return lax.broadcasted_iota(jnp.int32, (n, n), 0), lax.broadcasted_iota(jnp.int32, (n, n), 1)


def to_col(row):
    n = row.shape[1]
    down, across = square(n)
    return jnp.sum(jnp.where(down == across, row, jnp.zeros((), row.dtype)), axis=1, keepdims=True)


def slot_onehot(group_row, per_group):
    down, across = square(group_row.shape[1])
    group_col = to_col(group_row)
    earlier = jnp.where((group_col == group_row) & (across < down), 1.0, 0.0)
    rank = jnp.sum(earlier, axis=1, keepdims=True)
    slot = (group_col * float(per_group) + rank).astype(jnp.int32)
    return jnp.where(slot == across, 1.0, 0.0).astype(bf16)


def group_of(ids, fs, tp):
    group = jnp.zeros(ids.shape, f32)
    for bound in range(1, fs):
        group = group + jnp.where(ids >= bound * tp, 1.0, 0.0)
    return group


def prep_kernel(fs, tp, tok_ref, ids_ref, weight_ref, out_ref):
    count, width = tok_ref.shape
    group = group_of(ids_ref[0:1, :], fs, tp)
    onehot = slot_onehot(group, count // fs)
    wide = tok_ref[...].astype(f32)
    scale = lax.rsqrt(jnp.mean(wide * wide, axis=-1, keepdims=True) + norm_eps)
    normed = (wide * scale).astype(bf16)
    lane = lax.broadcasted_iota(jnp.int32, (count, lanes), 1)
    extra = jnp.zeros((count, lanes), f32)
    for pick in range(2):
        local = ids_ref[pick : pick + 1, :].astype(f32) - group * float(tp)
        local = to_col(local).astype(jnp.int32)
        rest = to_col(weight_ref[pick : pick + 1, :])
        for part in range(3):
            piece = rest.astype(bf16).astype(f32)
            extra = extra + jnp.where(lane == local + part * tp, piece, 0.0)
            rest = rest - piece
    dims = (((0,), (0,)), ((), ()))
    out_ref[:, :width] = lax.dot_general(onehot, normed, dims, preferred_element_type=f32).astype(bf16)
    out_ref[:, width:] = lax.dot_general(
        onehot, extra.astype(bf16), dims, preferred_element_type=f32
    ).astype(bf16)


def cast_kernel(steps, scaled, squeeze, me_ref, in_ref, *refs):
    step = pl.program_id(0)
    value = in_ref[:, 0] if squeeze else in_ref[0]
    if scaled:
        value = value * to_col(refs[0][...])[None]
        refs = refs[1:]
    value = value.astype(bf16)
    for r in range(steps):

        @pl.when(step == r)
        def _(r=r):
            refs[r][...] = value


def cast_along(me, matrix, scale, axis):
    fs, tp, rows, cols = matrix.shape
    steps = (fs, tp)[axis]
    if axis == 0:
        in_spec = pl.BlockSpec((1, tp, rows, cols), lambda r, m: (lax.rem(m[0] + r, fs), 0, 0, 0))
        shape = (tp, rows, cols)
    else:
        in_spec = pl.BlockSpec((fs, 1, rows, cols), lambda r, m: (0, lax.rem(m[1] + r, tp), 0, 0))
        shape = (fs, rows, cols)
    in_specs, args = [in_spec], [matrix]
    if scale is not None:
        in_specs.append(whole(scale.shape))
        args.append(scale)
    return pl.pallas_call(
        functools.partial(cast_kernel, steps, scale is not None, axis == 1),
        grid_spec=pltpu.PrefetchScalarGridSpec(
            num_scalar_prefetch=1, grid=(steps,), in_specs=in_specs, out_specs=[whole(shape)] * steps
        ),
        out_shape=[jax.ShapeDtypeStruct(shape, bf16)] * steps,
        compiler_params=params(),
        cost_estimate=cost(1e9, 6 * matrix.size),
    )(me, *args)


def in_order(me_ref, tp, action):
    for value in range(tp):

        @pl.when(me_ref[1] == value)
        def _(value=value):
            action([(value - j) % tp for j in range(tp)])


def merge_kernel(tp, me_ref, *refs):
    out_ref = refs[tp]

    def store(order):
        out_ref[0] = jnp.concatenate([refs[q][0] for q in order], axis=-1)

    in_order(me_ref, tp, store)


def merge(me, parts):
    tp = len(parts)
    fs, rows, cols = parts[0].shape
    return pl.pallas_call(
        functools.partial(merge_kernel, tp),
        grid_spec=pltpu.PrefetchScalarGridSpec(
            num_scalar_prefetch=1,
            grid=(fs,),
            in_specs=[pl.BlockSpec((1, rows, cols), lambda g, m: (g, 0, 0))] * tp,
            out_specs=pl.BlockSpec((1, rows, tp * cols), lambda g, m: (g, 0, 0)),
        ),
        out_shape=jax.ShapeDtypeStruct((fs, rows, tp * cols), bf16),
        compiler_params=params(),
        cost_estimate=cost(1e9, 4 * tp * parts[0].size),
    )(me, *parts)


def merge_down_kernel(fs, tp, first, me_ref, *refs):
    ins, outs = refs[:tp], refs[tp:]

    def store(order):
        for r in range(fs):
            group = lax.rem(me_ref[0] + r, fs)
            full = jnp.concatenate([ins[q][group] for q in order], axis=-1)
            outs[r][...] = full[:, :first]
            outs[fs][group] = full[:, first:]

    in_order(me_ref, tp, store)


def merge_down(me, parts, first):
    tp = len(parts)
    fs, rows, cols = parts[0].shape
    shapes = [(rows, first)] * fs + [(fs, rows, tp * cols - first)]
    outs = pl.pallas_call(
        functools.partial(merge_down_kernel, fs, tp, first),
        grid_spec=pltpu.PrefetchScalarGridSpec(
            num_scalar_prefetch=1,
            grid=(1,),
            in_specs=[whole(parts[0].shape)] * tp,
            out_specs=[whole(shape) for shape in shapes],
        ),
        out_shape=[jax.ShapeDtypeStruct(shape, bf16) for shape in shapes],
        compiler_params=params(),
        cost_estimate=cost(1e9, 4 * tp * parts[0].size),
    )(me, *parts)
    return outs[:fs], outs[fs]


def regroup_kernel(fs, tp, me_ref, *refs):
    for q in range(tp):
        target = lax.rem(me_ref[1] + q, tp)
        for r in range(fs):
            refs[fs + q][r] = refs[r][target]


def regroup(me, parts):
    fs = len(parts)
    tp, rows, cols = parts[0].shape
    shape = (fs, rows, cols)
    return pl.pallas_call(
        functools.partial(regroup_kernel, fs, tp),
        grid_spec=pltpu.PrefetchScalarGridSpec(
            num_scalar_prefetch=1,
            grid=(1,),
            in_specs=[whole(parts[0].shape)] * fs,
            out_specs=[whole(shape)] * tp,
        ),
        out_shape=[jax.ShapeDtypeStruct(shape, bf16)] * tp,
        compiler_params=params(),
        cost_estimate=cost(1e9, 4 * fs * parts[0].size),
    )(me, *parts)


def product_of(x_refs, matrix_ref, rows_ref):
    width = matrix_ref.shape[0]
    count = x_refs[0].shape[0]
    for q, ref in enumerate(x_refs):
        rows_ref[q * count : (q + 1) * count, :] = ref[:, :width]
    return jnp.dot(rows_ref[...], matrix_ref[...], preferred_element_type=f32)


def gate_kernel(fs, tp, me_ref, *refs):
    x_refs, parts, (matrix_ref, out_ref, rows_ref) = refs[:tp], refs[tp : 2 * tp], refs[2 * tp :]
    height = parts[0].shape[1]

    def store(order):
        for r in range(fs):
            origin = lax.rem(me_ref[0] - r + fs, fs)
            matrix_ref[pl.ds(pl.multiple_of(origin * height, height), height), :] = jnp.concatenate(
                [parts[q][r] for q in order], axis=-1
            )

    in_order(me_ref, tp, store)
    out_ref[...] = product_of(x_refs, matrix_ref, rows_ref)


def gate_rows(me, rows, parts):
    tp = len(parts)
    fs, height, cols = parts[0].shape
    matrix = (fs * height, tp * cols)
    out = (tp * rows[0].shape[0], tp * cols)
    return pl.pallas_call(
        functools.partial(gate_kernel, fs, tp),
        grid_spec=pltpu.PrefetchScalarGridSpec(
            num_scalar_prefetch=1,
            grid=(1,),
            in_specs=[whole(rows[0].shape)] * tp + [whole(parts[0].shape)] * tp,
            out_specs=[whole(matrix), whole(out)],
            scratch_shapes=[pltpu.VMEM((out[0], matrix[0]), bf16)],
        ),
        out_shape=[jax.ShapeDtypeStruct(matrix, bf16), jax.ShapeDtypeStruct(out, f32)],
        compiler_params=params(),
        cost_estimate=cost(2 * out[0] * matrix[0] * matrix[1], 4 * matrix[0] * matrix[1]),
    )(me, *rows, *parts)


def up_kernel(tp, *refs):
    x_refs, (matrix_ref, gate_ref, out_ref, rows_ref) = refs[:tp], refs[tp:]
    up = product_of(x_refs, matrix_ref, rows_ref)
    gate = gate_ref[...]
    out_ref[...] = (gate / (1.0 + jnp.exp(-gate)) * up).astype(bf16)


def up_rows(rows, matrix, gate):
    tp = len(rows)
    return pl.pallas_call(
        functools.partial(up_kernel, tp),
        grid=(1,),
        in_specs=[whole(rows[0].shape)] * tp + [whole(matrix.shape), whole(gate.shape)],
        out_specs=whole(gate.shape),
        scratch_shapes=[pltpu.VMEM((gate.shape[0], matrix.shape[0]), bf16)],
        out_shape=jax.ShapeDtypeStruct(gate.shape, bf16),
        compiler_params=params(),
        cost_estimate=cost(2 * gate.size * matrix.shape[0], 2 * matrix.size),
    )(*rows, matrix, gate)


def down_kernel(fs, tp, parts_count, aliased, me_ref, hidden_ref, *refs):
    w_refs, refs = refs[:tp], refs[tp:]
    parts, refs = refs[:parts_count], refs[parts_count:]
    if aliased:
        refs = refs[1:]
    matrix_ref, outs = refs[0], refs[1:]
    if parts_count == 1:
        matrix_ref[...] = parts[0][...]
    else:
        rows = parts[0].shape[0]
        for r in range(fs):
            origin = lax.rem(me_ref[0] - r + fs, fs)
            matrix_ref[pl.ds(pl.multiple_of(origin * rows, rows), rows), :] = parts[r][...]
    product = jnp.dot(hidden_ref[...], matrix_ref[...], preferred_element_type=f32)
    product = product.astype(bf16).astype(f32)
    count = w_refs[0].shape[0]
    lane = lax.broadcasted_iota(jnp.int32, (count, lanes), 1)
    mine = me_ref[1]
    chosen = (lane == mine) | (lane == mine + tp) | (lane == mine + 2 * tp)
    for q in range(tp):
        weight = jnp.sum(
            jnp.where(chosen, w_refs[q][...].astype(f32), 0.0), axis=1, keepdims=True
        )
        outs[q][...] = (product[q * count : (q + 1) * count] * weight).astype(bf16)


def down_rows(me, fs, hidden, rows, parts, low, width, prior):
    tp = len(rows)
    count = rows[0].shape[0]
    depth = hidden.shape[1]
    size = parts[0].shape[1]
    col_block = low // size
    weight_block = width // lanes
    in_specs = [whole(hidden.shape)]
    in_specs += [pl.BlockSpec((count, lanes), lambda k, m: (0, weight_block))] * tp
    in_specs += [whole(part.shape) for part in parts]
    args = [hidden, *rows, *parts]
    aliases = {}
    if prior is not None:
        in_specs.append(pl.BlockSpec(memory_space=pl.ANY))
        args.append(prior)
        aliases = {len(args): 0}
    outs = pl.pallas_call(
        functools.partial(down_kernel, fs, tp, len(parts), prior is not None),
        grid_spec=pltpu.PrefetchScalarGridSpec(
            num_scalar_prefetch=1,
            grid=(1,),
            in_specs=in_specs,
            out_specs=[pl.BlockSpec((depth, size), lambda k, m: (0, col_block))]
            + [whole((count, size))] * tp,
        ),
        out_shape=[jax.ShapeDtypeStruct((depth, width), bf16)]
        + [jax.ShapeDtypeStruct((count, size), bf16)] * tp,
        input_output_aliases=aliases,
        compiler_params=params(),
        cost_estimate=cost(2 * tp * count * depth * size, 4 * depth * size),
    )(me, *args)
    return outs[0], outs[1:]


def final_kernel(fs, tp, ids_ref, *refs):
    out_ref = refs[-1]
    onehot = slot_onehot(group_of(ids_ref[0:1, :], fs, tp), ids_ref.shape[1] // fs)
    low = 0
    for ref in refs[:-1]:
        high = low + ref.shape[1]
        out_ref[:, low:high] = jnp.dot(onehot, ref[...], preferred_element_type=f32).astype(bf16)
        low = high


def shards(tokens, norm_gain, gate_proj, up_proj, down_proj, expert_ids, route_weight):
    fs = lax.axis_size("fs")
    tp = lax.axis_size("tp")
    me = jnp.stack([lax.axis_index("fs"), lax.axis_index("tp")]).astype(jnp.int32)
    count, width = tokens.shape
    per_group = count // fs
    first = width // 2

    def shift(n, step):
        return [(k, (k + step) % n) for k in range(n)]

    def rotate(parts, axis, back=False):
        n = len(parts)
        return [parts[0]] + [
            lax.ppermute(parts[r], axis, shift(n, n - r if back else r)) for r in range(1, n)
        ]

    def swap_fs(value):
        return lax.all_to_all(value, "fs", 0, 0, tiled=True)

    def by_expert(matrix):
        return matrix.reshape((fs, tp) + matrix.shape[1:])

    ids, weights = expert_ids.T, route_weight.T
    scale = norm_gain[None, :]

    sorted_rows = pl.pallas_call(
        functools.partial(prep_kernel, fs, tp),
        out_shape=jax.ShapeDtypeStruct((count, width + lanes), bf16),
        compiler_params=params(),
        cost_estimate=cost(2 * count * count * width, 4 * count * width),
    )(tokens, ids, weights)
    landed = swap_fs(sorted_rows.reshape(fs, per_group, width + lanes))
    landed = landed.reshape(count, width + lanes)
    gate_parts = cast_along(me, by_expert(gate_proj), scale, 0)
    gate_parts = rotate(gate_parts, "fs")
    up_parts = cast_along(me, by_expert(up_proj), scale, 1)
    up_parts = rotate(up_parts, "tp")
    rows = rotate([landed] * tp, "tp")
    up_here = merge(me, up_parts)
    new_up = swap_fs(up_here)
    new_up = new_up.reshape(-1, new_up.shape[2])
    down_parts = cast_along(me, by_expert(down_proj), None, 1)
    down_parts = rotate(down_parts, "tp")
    gate_parts = regroup(me, gate_parts)
    gate_parts = rotate(gate_parts, "tp")
    down_first, down_last = merge_down(me, down_parts, first)
    down_first = rotate(down_first, "fs")
    new_gate, gate = gate_rows(me, rows, gate_parts)
    down_last = swap_fs(down_last)
    down_last = down_last.reshape(-1, down_last.shape[2])
    hidden = up_rows(rows, new_up, gate)

    def add(parts):
        return sum(part.astype(f32) for part in parts).astype(bf16)

    def back_fs(value):
        return swap_fs(value.reshape(fs, per_group, -1)).reshape(count, -1)

    new_down, partial = down_rows(me, fs, hidden, rows, down_first, 0, width, None)
    partial = rotate(partial, "tp", back=True)
    back_first = back_fs(add(partial))
    new_down, partial = down_rows(me, fs, hidden, rows, [down_last], first, width, new_down)
    partial = rotate(partial, "tp", back=True)
    back_last = back_fs(add(partial))
    mixed = pl.pallas_call(
        functools.partial(final_kernel, fs, tp),
        out_shape=jax.ShapeDtypeStruct((count, width), bf16),
        compiler_params=params(),
        cost_estimate=cost(2 * count * count * width, 4 * count * width),
    )(ids, back_first, back_last)
    return (mixed, new_gate[None], new_up[None], new_down[None])


def solution(mesh):
    in_specs = (
        P(("fs", "tp"), None),
        P("fs"),
        P(None, "fs", "tp"),
        P(None, "fs", "tp"),
        P(None, "fs", "tp"),
        P(("fs", "tp"), None),
        P(("fs", "tp"), None),
    )
    out_specs = (
        P(("fs", "tp"), None),
        P(("fs", "tp"), None, None),
        P(("fs", "tp"), None, None),
        P(("fs", "tp"), None, None),
    )

    return jax.shard_map(shards, mesh=mesh, in_specs=in_specs, out_specs=out_specs, check_vma=False)
```

```python
import functools

import jax
import jax.numpy as jnp
from jax import lax
from jax.experimental import pallas as pl
from jax.experimental.pallas import tpu as pltpu
from jax.sharding import PartitionSpec as P


norm_eps = 1e-06
lanes = 128
bf16 = jnp.bfloat16
f32 = jnp.float32
small = pltpu.CompilerParams(vmem_limit_bytes=16 * 1024 * 1024)


def cuts_of(width):
    half, rest = width // 2, width // 2 + width // 4
    return [(0, half), (half, rest), (rest, width)]


returns = [(0, 1), (2,)]


def cost(flops, nbytes):
    return pl.CostEstimate(flops=int(flops), bytes_accessed=int(nbytes), transcendentals=0)


def whole(shape):
    return pl.BlockSpec(shape, lambda *_: (0,) * len(shape))


def square(n):
    return lax.broadcasted_iota(jnp.int32, (n, n), 0), lax.broadcasted_iota(jnp.int32, (n, n), 1)


def to_col(row):
    n = row.shape[1]
    down, across = square(n)
    return jnp.sum(jnp.where(down == across, row, jnp.zeros((), row.dtype)), axis=1, keepdims=True)


def slot_onehot(group_row, me, fs):
    count = group_row.shape[1]
    down, across = square(count)
    group_col = to_col(group_row)
    earlier = jnp.where((group_col == group_row) & (across < down), 1.0, 0.0)
    rank = jnp.sum(earlier, axis=1, keepdims=True).astype(jnp.int32)
    ahead = group_col.astype(jnp.int32) - me
    ahead = jnp.where(ahead < 0, ahead + fs, ahead)
    slot = ahead * (count // fs) + rank
    return jnp.where(slot == across, 1.0, 0.0).astype(bf16)


def group_of(ids, fs, tp):
    group = jnp.zeros(ids.shape, f32)
    for bound in range(1, fs):
        group = group + jnp.where(ids >= bound * tp, 1.0, 0.0)
    return group


def prep_kernel(fs, tp, me_ref, tok_ref, ids_ref, weight_ref, *outs):
    count, width = tok_ref.shape
    group = group_of(ids_ref[0:1, :], fs, tp)
    onehot = slot_onehot(group, me_ref[0], fs)
    wide = tok_ref[...].astype(f32)
    scale = lax.rsqrt(jnp.mean(wide * wide, axis=-1, keepdims=True) + norm_eps)
    normed = (wide * scale).astype(bf16)
    lane = lax.broadcasted_iota(jnp.int32, (count, lanes), 1)
    extra = jnp.zeros((count, lanes), f32)
    for pick in range(2):
        local = ids_ref[pick : pick + 1, :].astype(f32) - group * float(tp)
        local = to_col(local).astype(jnp.int32)
        rest = to_col(weight_ref[pick : pick + 1, :])
        for part in range(3):
            piece = rest.astype(bf16).astype(f32)
            extra = extra + jnp.where(lane == local + part * tp, piece, 0.0)
            rest = rest - piece
    dims = (((0,), (0,)), ((), ()))
    rows = lax.dot_general(onehot, normed, dims, preferred_element_type=f32).astype(bf16)
    extra = lax.dot_general(onehot, extra.astype(bf16), dims, preferred_element_type=f32).astype(bf16)
    each = count // fs
    for r in range(fs):
        outs[r][:, :width] = rows[r * each : (r + 1) * each]
        outs[r][:, width:] = extra[r * each : (r + 1) * each]


def join_kernel(*refs):
    each = refs[0].shape[0]
    for r, ref in enumerate(refs[:-1]):
        refs[-1][r * each : (r + 1) * each, :] = ref[...]


def join(parts):
    each, width = parts[0].shape
    return pl.pallas_call(
        join_kernel,
        out_shape=jax.ShapeDtypeStruct((each * len(parts), width), bf16),
        compiler_params=small,
        cost_estimate=cost(1e9, 4 * len(parts) * parts[0].size),
    )(*parts)


def add_kernel(fs, tp, *refs):
    ins, outs = refs[:-fs], refs[-fs:]
    each = outs[0].shape[0]
    low = 0
    for k in range(0, len(ins), tp):
        total = sum(ref[...].astype(f32) for ref in ins[k : k + tp]).astype(bf16)
        high = low + total.shape[1]
        for r in range(fs):
            outs[r][:, low:high] = total[r * each : (r + 1) * each]
        low = high


def add(fs, groups):
    tp = len(groups[0])
    count = groups[0][0].shape[0]
    width = sum(group[0].shape[1] for group in groups)
    return pl.pallas_call(
        functools.partial(add_kernel, fs, tp),
        out_shape=[jax.ShapeDtypeStruct((count // fs, width), bf16)] * fs,
        compiler_params=small,
        cost_estimate=cost(1e9, 2 * (tp + 1) * count * width),
    )(*[part for group in groups for part in group])


def cast_kernel(steps, scaled, squeeze, me_ref, in_ref, *refs):
    step = pl.program_id(0)
    value = in_ref[:, 0] if squeeze else in_ref[0]
    if scaled:
        value = value * to_col(refs[0][...])[None]
        refs = refs[1:]
    value = value.astype(bf16)
    for r in range(steps):

        @pl.when(step == r)
        def _(r=r):
            refs[r][...] = value


def cast_along(me, matrix, scale, axis):
    fs, tp, rows, cols = matrix.shape
    steps = (fs, tp)[axis]
    if axis == 0:
        in_spec = pl.BlockSpec((1, tp, rows, cols), lambda r, m: (lax.rem(m[0] + r, fs), 0, 0, 0))
        shape = (tp, rows, cols)
    else:
        in_spec = pl.BlockSpec((fs, 1, rows, cols), lambda r, m: (0, lax.rem(m[1] + r, tp), 0, 0))
        shape = (fs, rows, cols)
    in_specs, args = [in_spec], [matrix]
    if scale is not None:
        in_specs.append(whole(scale.shape))
        args.append(scale)
    return pl.pallas_call(
        functools.partial(cast_kernel, steps, scale is not None, axis == 1),
        grid_spec=pltpu.PrefetchScalarGridSpec(
            num_scalar_prefetch=1, grid=(steps,), in_specs=in_specs, out_specs=[whole(shape)] * steps
        ),
        out_shape=[jax.ShapeDtypeStruct(shape, bf16)] * steps,
        cost_estimate=cost(1e9, 6 * matrix.size),
    )(me, *args)


def in_order(me_ref, tp, action):
    for value in range(tp):

        @pl.when(me_ref[1] == value)
        def _(value=value):
            action([(value - j) % tp for j in range(tp)])


def merge_kernel(tp, me_ref, *refs):
    out_ref = refs[tp]

    def store(order):
        out_ref[0] = jnp.concatenate([refs[q][0] for q in order], axis=-1)

    in_order(me_ref, tp, store)


def merge(me, parts):
    tp = len(parts)
    fs, rows, cols = parts[0].shape
    return pl.pallas_call(
        functools.partial(merge_kernel, tp),
        grid_spec=pltpu.PrefetchScalarGridSpec(
            num_scalar_prefetch=1,
            grid=(fs,),
            in_specs=[pl.BlockSpec((1, rows, cols), lambda g, m: (g, 0, 0))] * tp,
            out_specs=pl.BlockSpec((1, rows, tp * cols), lambda g, m: (g, 0, 0)),
        ),
        out_shape=jax.ShapeDtypeStruct((fs, rows, tp * cols), bf16),
        cost_estimate=cost(1e9, 4 * tp * parts[0].size),
    )(me, *parts)


def merge_down_kernel(fs, tp, cuts, me_ref, *refs):
    ins, outs = refs[:tp], refs[tp:]

    def store(order):
        for r in range(fs):
            group = lax.rem(me_ref[0] + r, fs)
            full = jnp.concatenate([ins[q][group] for q in order], axis=-1)
            for k, (low, high) in enumerate(cuts):
                outs[k * fs + r][...] = full[:, low:high]

    in_order(me_ref, tp, store)


def merge_down(me, parts, cuts):
    tp = len(parts)
    fs, rows, _ = parts[0].shape
    shapes = [(rows, high - low) for low, high in cuts for _ in range(fs)]
    outs = pl.pallas_call(
        functools.partial(merge_down_kernel, fs, tp, cuts),
        grid_spec=pltpu.PrefetchScalarGridSpec(
            num_scalar_prefetch=1,
            grid=(1,),
            in_specs=[whole(parts[0].shape)] * tp,
            out_specs=[whole(shape) for shape in shapes],
        ),
        out_shape=[jax.ShapeDtypeStruct(shape, bf16) for shape in shapes],
        cost_estimate=cost(1e9, 4 * tp * parts[0].size),
    )(me, *parts)
    return [outs[k * fs : (k + 1) * fs] for k in range(len(cuts))]


def regroup_kernel(fs, tp, me_ref, *refs):
    for q in range(tp):
        target = lax.rem(me_ref[1] + q, tp)
        for r in range(fs):
            refs[fs + q][r] = refs[r][target]


def regroup(me, parts):
    fs = len(parts)
    tp, rows, cols = parts[0].shape
    shape = (fs, rows, cols)
    return pl.pallas_call(
        functools.partial(regroup_kernel, fs, tp),
        grid_spec=pltpu.PrefetchScalarGridSpec(
            num_scalar_prefetch=1,
            grid=(1,),
            in_specs=[whole(parts[0].shape)] * fs,
            out_specs=[whole(shape)] * tp,
        ),
        out_shape=[jax.ShapeDtypeStruct(shape, bf16)] * tp,
        cost_estimate=cost(1e9, 4 * fs * parts[0].size),
    )(me, *parts)


def product_of(x_refs, matrix_ref, rows_ref):
    width = matrix_ref.shape[0]
    count = x_refs[0].shape[0]
    for q, ref in enumerate(x_refs):
        rows_ref[q * count : (q + 1) * count, :] = ref[:, :width]
    return jnp.dot(rows_ref[...], matrix_ref[...], preferred_element_type=f32)


def gate_kernel(fs, tp, me_ref, *refs):
    x_refs, parts, (matrix_ref, out_ref, rows_ref) = refs[:tp], refs[tp : 2 * tp], refs[2 * tp :]
    height = parts[0].shape[1]

    def store(order):
        for r in range(fs):
            origin = lax.rem(me_ref[0] - r + fs, fs)
            matrix_ref[pl.ds(pl.multiple_of(origin * height, height), height), :] = jnp.concatenate(
                [parts[q][r] for q in order], axis=-1
            )

    in_order(me_ref, tp, store)
    out_ref[...] = product_of(x_refs, matrix_ref, rows_ref)


def gate_rows(me, rows, parts):
    tp = len(parts)
    fs, height, cols = parts[0].shape
    matrix = (fs * height, tp * cols)
    out = (tp * rows[0].shape[0], tp * cols)
    return pl.pallas_call(
        functools.partial(gate_kernel, fs, tp),
        grid_spec=pltpu.PrefetchScalarGridSpec(
            num_scalar_prefetch=1,
            grid=(1,),
            in_specs=[whole(rows[0].shape)] * tp + [whole(parts[0].shape)] * tp,
            out_specs=[whole(matrix), whole(out)],
            scratch_shapes=[pltpu.VMEM((out[0], matrix[0]), bf16)],
        ),
        out_shape=[jax.ShapeDtypeStruct(matrix, bf16), jax.ShapeDtypeStruct(out, f32)],
        cost_estimate=cost(2 * out[0] * matrix[0] * matrix[1], 4 * matrix[0] * matrix[1]),
    )(me, *rows, *parts)


def up_kernel(tp, *refs):
    x_refs, (in_ref, gate_ref, matrix_ref, out_ref, rows_ref) = refs[:tp], refs[tp:]
    matrix_ref[...] = in_ref[...]
    up = product_of(x_refs, in_ref, rows_ref)
    gate = gate_ref[...]
    out_ref[...] = (gate / (1.0 + jnp.exp(-gate)) * up).astype(bf16)


def up_rows(rows, matrix, gate):
    tp = len(rows)
    return pl.pallas_call(
        functools.partial(up_kernel, tp),
        grid=(1,),
        in_specs=[whole(rows[0].shape)] * tp + [whole(matrix.shape), whole(gate.shape)],
        out_specs=[whole(matrix.shape), whole(gate.shape)],
        scratch_shapes=[pltpu.VMEM((gate.shape[0], matrix.shape[0]), bf16)],
        out_shape=[
            jax.ShapeDtypeStruct(matrix.shape, bf16),
            jax.ShapeDtypeStruct(gate.shape, bf16),
        ],
        cost_estimate=cost(2 * gate.size * matrix.shape[0], 4 * matrix.size),
    )(*rows, matrix, gate)


def down_kernel(fs, tp, parts_count, aliased, me_ref, hidden_ref, *refs):
    w_refs, refs = refs[:tp], refs[tp:]
    parts, refs = refs[:parts_count], refs[parts_count:]
    if aliased:
        refs = refs[1:]
    matrix_ref, outs = refs[0], refs[1:]
    if parts_count == 1:
        matrix_ref[...] = parts[0][...]
    else:
        rows = parts[0].shape[0]
        for r in range(fs):
            origin = lax.rem(me_ref[0] - r + fs, fs)
            matrix_ref[pl.ds(pl.multiple_of(origin * rows, rows), rows), :] = parts[r][...]
    product = jnp.dot(hidden_ref[...], matrix_ref[...], preferred_element_type=f32)
    product = product.astype(bf16).astype(f32)
    count = w_refs[0].shape[0]
    lane = lax.broadcasted_iota(jnp.int32, (count, lanes), 1)
    mine = me_ref[1]
    chosen = (lane == mine) | (lane == mine + tp) | (lane == mine + 2 * tp)
    for q in range(tp):
        weight = jnp.sum(
            jnp.where(chosen, w_refs[q][...].astype(f32), 0.0), axis=1, keepdims=True
        )
        outs[q][...] = (product[q * count : (q + 1) * count] * weight).astype(bf16)


def down_rows(me, fs, hidden, rows, parts, low, width, prior):
    tp = len(rows)
    count = rows[0].shape[0]
    depth = hidden.shape[1]
    size = parts[0].shape[1]
    col_block = low // size
    weight_block = width // lanes
    in_specs = [whole(hidden.shape)]
    in_specs += [pl.BlockSpec((count, lanes), lambda k, m: (0, weight_block))] * tp
    in_specs += [whole(part.shape) for part in parts]
    args = [hidden, *rows, *parts]
    aliases = {}
    if prior is not None:
        in_specs.append(pl.BlockSpec(memory_space=pl.ANY))
        args.append(prior)
        aliases = {len(args): 0}
    outs = pl.pallas_call(
        functools.partial(down_kernel, fs, tp, len(parts), prior is not None),
        grid_spec=pltpu.PrefetchScalarGridSpec(
            num_scalar_prefetch=1,
            grid=(1,),
            in_specs=in_specs,
            out_specs=[pl.BlockSpec((depth, size), lambda k, m: (0, col_block))]
            + [whole((count, size))] * tp,
        ),
        out_shape=[jax.ShapeDtypeStruct((depth, width), bf16)]
        + [jax.ShapeDtypeStruct((count, size), bf16)] * tp,
        input_output_aliases=aliases,
        compiler_params=small,
        cost_estimate=cost(2 * tp * count * depth * size, 4 * depth * size),
    )(me, *args)
    return outs[0], outs[1:]


def final_kernel(fs, tp, me_ref, ids_ref, *refs):
    ins, out_ref = refs[:-1], refs[-1]
    onehot = slot_onehot(group_of(ids_ref[0:1, :], fs, tp), me_ref[0], fs)
    low = 0
    for k in range(0, len(ins), fs):
        back = jnp.concatenate([ref[...] for ref in ins[k : k + fs]], axis=0)
        high = low + back.shape[1]
        out_ref[:, low:high] = jnp.dot(onehot, back, preferred_element_type=f32).astype(bf16)
        low = high


def shards(tokens, norm_gain, gate_proj, up_proj, down_proj, expert_ids, route_weight):
    fs = lax.axis_size("fs")
    tp = lax.axis_size("tp")
    me = jnp.stack([lax.axis_index("fs"), lax.axis_index("tp")]).astype(jnp.int32)
    count, width = tokens.shape
    cuts = cuts_of(width)
    in_smem = pl.BlockSpec(memory_space=pltpu.SMEM)
    in_vmem = pl.BlockSpec(memory_space=pltpu.VMEM)

    def rotate(parts, axis, back=False):
        n = len(parts)
        out = [parts[0]]
        for r in range(1, n):
            step = n - r if back else r
            out.append(lax.ppermute(parts[r], axis, [(k, (k + step) % n) for k in range(n)]))
        return out

    def by_expert(matrix):
        return matrix.reshape((fs, tp) + matrix.shape[1:])

    ids, weights = expert_ids.T, route_weight.T
    scale = norm_gain[None, :]

    gate_parts = cast_along(me, by_expert(gate_proj), scale, 0)
    gate_parts = rotate(gate_parts, "fs")
    up_parts = cast_along(me, by_expert(up_proj), scale, 1)
    up_parts = rotate(up_parts, "tp")
    sent = pl.pallas_call(
        functools.partial(prep_kernel, fs, tp),
        in_specs=[in_smem, in_vmem, in_vmem, in_vmem],
        out_shape=[jax.ShapeDtypeStruct((count // fs, width + lanes), bf16)] * fs,
        cost_estimate=cost(2 * count * count * width, 4 * count * width),
    )(me, tokens, ids, weights)
    landed = rotate(sent, "fs")
    down_parts = cast_along(me, by_expert(down_proj), None, 1)
    down_parts = rotate(down_parts, "tp")
    up_here = merge(me, up_parts)
    up_here = lax.all_to_all(up_here, "fs", 0, 0, tiled=True)
    up_here = up_here.reshape(-1, up_here.shape[2])
    gate_parts = regroup(me, gate_parts)
    gate_parts = rotate(gate_parts, "tp")
    landed = join(landed)
    rows = rotate([landed] * tp, "tp")
    down_parts = merge_down(me, down_parts, cuts)
    for k in range(len(cuts)):
        down_parts[k] = rotate(down_parts[k], "fs")
    new_gate, gate = gate_rows(me, rows, gate_parts)
    new_up, hidden = up_rows(rows, up_here, gate)
    new_down = None
    partials = []
    for k, (low, _) in enumerate(cuts):
        new_down, partial = down_rows(
            me, fs, hidden, rows, down_parts[k], low, width, new_down
        )
        partials.append(rotate(partial, "tp", back=True))
    backs = []
    for members in returns:
        summed = add(fs, [partials[m] for m in members])
        backs += rotate(summed, "fs", back=True)
    mixed = pl.pallas_call(
        functools.partial(final_kernel, fs, tp),
        in_specs=[in_smem] + [in_vmem] * (1 + len(backs)),
        out_shape=jax.ShapeDtypeStruct((count, width), bf16),
        compiler_params=small,
        cost_estimate=cost(2 * count * count * width, 4 * count * width),
    )(me, ids, *backs)
    return (mixed, new_gate[None], new_up[None], new_down[None])


def solution(mesh):
    in_specs = (
        P(("fs", "tp"), None),
        P("fs"),
        P(None, "fs", "tp"),
        P(None, "fs", "tp"),
        P(None, "fs", "tp"),
        P(("fs", "tp"), None),
        P(("fs", "tp"), None),
    )
    out_specs = (
        P(("fs", "tp"), None),
        P(("fs", "tp"), None, None),
        P(("fs", "tp"), None, None),
        P(("fs", "tp"), None, None),
    )

    return jax.shard_map(shards, mesh=mesh, in_specs=in_specs, out_specs=out_specs, check_vma=False)
```

```python
import functools

import jax
import jax.numpy as jnp
from jax import lax
from jax.experimental import pallas as pl
from jax.experimental.pallas import tpu as pltpu
from jax.sharding import PartitionSpec as P


norm_eps = 1e-06
lanes = 128
bf16 = jnp.bfloat16
f32 = jnp.float32


def cuts_of(width):
    half, rest = width // 2, width - width // 8
    return [(0, half), (half, rest), (rest, width)]


returns = [(0,), (1, 2)]


def grant(mib):
    return pltpu.CompilerParams(vmem_limit_bytes=mib * 1024 * 1024)


def far_first(n):
    return sorted(range(1, n), key=lambda r: (abs(2 * r - n), r))


def cost(flops, nbytes):
    return pl.CostEstimate(flops=int(flops), bytes_accessed=int(nbytes), transcendentals=0)


def whole(shape):
    return pl.BlockSpec(shape, lambda *_: (0,) * len(shape))


def square(n):
    return lax.broadcasted_iota(jnp.int32, (n, n), 0), lax.broadcasted_iota(jnp.int32, (n, n), 1)


def to_col(row):
    n = row.shape[1]
    down, across = square(n)
    return jnp.sum(jnp.where(down == across, row, jnp.zeros((), row.dtype)), axis=1, keepdims=True)


def slot_onehot(group_row, me, fs):
    count = group_row.shape[1]
    down, across = square(count)
    group_col = to_col(group_row)
    earlier = jnp.where((group_col == group_row) & (across < down), 1.0, 0.0)
    rank = jnp.sum(earlier, axis=1, keepdims=True).astype(jnp.int32)
    ahead = group_col.astype(jnp.int32) - me
    ahead = jnp.where(ahead < 0, ahead + fs, ahead)
    slot = ahead * (count // fs) + rank
    return jnp.where(slot == across, 1.0, 0.0).astype(bf16)


def group_of(ids, fs, tp):
    group = jnp.zeros(ids.shape, f32)
    for bound in range(1, fs):
        group = group + jnp.where(ids >= bound * tp, 1.0, 0.0)
    return group


def prep_kernel(fs, tp, me_ref, tok_ref, ids_ref, weight_ref, *outs):
    count, width = tok_ref.shape
    group = group_of(ids_ref[0:1, :], fs, tp)
    onehot = slot_onehot(group, me_ref[0], fs)
    wide = tok_ref[...].astype(f32)
    scale = lax.rsqrt(jnp.mean(wide * wide, axis=-1, keepdims=True) + norm_eps)
    normed = (wide * scale).astype(bf16)
    lane = lax.broadcasted_iota(jnp.int32, (count, lanes), 1)
    extra = jnp.zeros((count, lanes), f32)
    for pick in range(2):
        local = ids_ref[pick : pick + 1, :].astype(f32) - group * float(tp)
        local = to_col(local).astype(jnp.int32)
        rest = to_col(weight_ref[pick : pick + 1, :])
        for part in range(3):
            piece = rest.astype(bf16).astype(f32)
            extra = extra + jnp.where(lane == local + part * tp, piece, 0.0)
            rest = rest - piece
    dims = (((0,), (0,)), ((), ()))
    rows = lax.dot_general(onehot, normed, dims, preferred_element_type=f32).astype(bf16)
    extra = lax.dot_general(onehot, extra.astype(bf16), dims, preferred_element_type=f32).astype(bf16)
    each = count // fs
    for r in range(fs):
        outs[r][:, :width] = rows[r * each : (r + 1) * each]
        outs[r][:, width:] = extra[r * each : (r + 1) * each]


def join_kernel(*refs):
    each = refs[0].shape[0]
    for r, ref in enumerate(refs[:-1]):
        refs[-1][r * each : (r + 1) * each, :] = ref[...]


def join(parts):
    each, width = parts[0].shape
    return pl.pallas_call(
        join_kernel,
        out_shape=jax.ShapeDtypeStruct((each * len(parts), width), bf16),
        compiler_params=grant(16),
        cost_estimate=cost(1e9, 4 * len(parts) * parts[0].size),
    )(*parts)


def add_kernel(tp, me_ref, *refs):
    ins, out_ref = refs[:-1], refs[-1]
    fs, each, _ = out_ref.shape
    low = 0
    for k in range(0, len(ins), tp):
        total = sum(ref[...].astype(f32) for ref in ins[k : k + tp]).astype(bf16)
        high = low + total.shape[1]
        for r in range(fs):
            out_ref[lax.rem(me_ref[0] - r + fs, fs), :, low:high] = total[r * each : (r + 1) * each]
        low = high


def add(me, fs, groups):
    tp = len(groups[0])
    count = groups[0][0].shape[0]
    width = sum(group[0].shape[1] for group in groups)
    terms = [part for group in groups for part in group]
    return pl.pallas_call(
        functools.partial(add_kernel, tp),
        in_specs=[pl.BlockSpec(memory_space=pltpu.SMEM)]
        + [pl.BlockSpec(memory_space=pltpu.VMEM)] * len(terms),
        out_shape=jax.ShapeDtypeStruct((fs, count // fs, width), bf16),
        compiler_params=grant(8),
        cost_estimate=cost(1e9, 2 * (tp + 1) * count * width),
    )(me, *terms)


def cast_kernel(steps, scaled, squeeze, me_ref, in_ref, *refs):
    step = pl.program_id(0)
    value = in_ref[:, 0] if squeeze else in_ref[0]
    if scaled:
        value = value * to_col(refs[0][...])[None]
        refs = refs[1:]
    value = value.astype(bf16)
    for k in range(steps):

        @pl.when(step == k)
        def _(k=k):
            refs[k][...] = value


def cast_along(me, matrix, scale, axis, distances, params):
    fs, tp, rows, cols = matrix.shape
    steps = len(distances)

    def target(k, m):
        ahead = jnp.int32(distances[0])
        for j in range(1, steps):
            ahead = jnp.where(k == j, jnp.int32(distances[j]), ahead)
        return lax.rem(m[axis] + ahead, (fs, tp)[axis])

    if axis == 0:
        in_spec = pl.BlockSpec((1, tp, rows, cols), lambda k, m: (target(k, m), 0, 0, 0))
        shape = (tp, rows, cols)
    else:
        in_spec = pl.BlockSpec((fs, 1, rows, cols), lambda k, m: (0, target(k, m), 0, 0))
        shape = (fs, rows, cols)
    in_specs, args = [in_spec], [matrix]
    if scale is not None:
        in_specs.append(whole(scale.shape))
        args.append(scale)
    return pl.pallas_call(
        functools.partial(cast_kernel, steps, scale is not None, axis == 1),
        grid_spec=pltpu.PrefetchScalarGridSpec(
            num_scalar_prefetch=1, grid=(steps,), in_specs=in_specs, out_specs=[whole(shape)] * steps
        ),
        out_shape=[jax.ShapeDtypeStruct(shape, bf16)] * steps,
        compiler_params=params,
        cost_estimate=cost(1e9, 6 * matrix.size * steps // (fs, tp)[axis]),
    )(me, *args)


def in_order(me_ref, tp, action):
    for value in range(tp):

        @pl.when(me_ref[1] == value)
        def _(value=value):
            action([(value - j) % tp for j in range(tp)])


def merge_kernel(fs, tp, cuts, me_ref, *refs):
    ins, outs = refs[:tp], refs[tp:]

    def store(order):
        for r in range(fs):
            group = lax.rem(me_ref[0] + r, fs)
            full = jnp.concatenate([ins[q][group] for q in order], axis=-1)
            for k, (low, high) in enumerate(cuts):
                outs[k * fs + r][...] = full[:, low:high]

    in_order(me_ref, tp, store)


def merge(me, parts, cuts):
    tp = len(parts)
    fs, rows, _ = parts[0].shape
    shapes = [(rows, high - low) for low, high in cuts for _ in range(fs)]
    outs = pl.pallas_call(
        functools.partial(merge_kernel, fs, tp, cuts),
        grid_spec=pltpu.PrefetchScalarGridSpec(
            num_scalar_prefetch=1,
            grid=(1,),
            in_specs=[whole(parts[0].shape)] * tp,
            out_specs=[whole(shape) for shape in shapes],
        ),
        out_shape=[jax.ShapeDtypeStruct(shape, bf16) for shape in shapes],
        compiler_params=grant(16),
        cost_estimate=cost(1e9, 4 * tp * parts[0].size),
    )(me, *parts)
    return [outs[k * fs : (k + 1) * fs] for k in range(len(cuts))]


def regroup_kernel(fs, tp, me_ref, *refs):
    for q in range(tp):
        target = lax.rem(me_ref[1] + q, tp)
        for r in range(fs):
            refs[fs + q][r] = refs[r][target]


def regroup(me, parts):
    fs = len(parts)
    tp, rows, cols = parts[0].shape
    shape = (fs, rows, cols)
    return pl.pallas_call(
        functools.partial(regroup_kernel, fs, tp),
        grid_spec=pltpu.PrefetchScalarGridSpec(
            num_scalar_prefetch=1,
            grid=(1,),
            in_specs=[whole(parts[0].shape)] * fs,
            out_specs=[whole(shape)] * tp,
        ),
        out_shape=[jax.ShapeDtypeStruct(shape, bf16)] * tp,
        compiler_params=grant(16),
        cost_estimate=cost(1e9, 4 * fs * parts[0].size),
    )(me, *parts)


def product_of(x_refs, matrix_ref, rows_ref):
    width = matrix_ref.shape[0]
    count = x_refs[0].shape[0]
    for q, ref in enumerate(x_refs):
        rows_ref[q * count : (q + 1) * count, :] = ref[:, :width]
    return jnp.dot(rows_ref[...], matrix_ref[...], preferred_element_type=f32)


def gate_kernel(fs, tp, me_ref, *refs):
    x_refs, parts, (matrix_ref, out_ref, rows_ref) = refs[:tp], refs[tp : 2 * tp], refs[2 * tp :]
    height = parts[0].shape[1]

    def store(order):
        for r in range(fs):
            origin = lax.rem(me_ref[0] - r + fs, fs)
            matrix_ref[pl.ds(pl.multiple_of(origin * height, height), height), :] = jnp.concatenate(
                [parts[q][r] for q in order], axis=-1
            )

    in_order(me_ref, tp, store)
    out_ref[...] = product_of(x_refs, matrix_ref, rows_ref)


def gate_rows(me, rows, parts):
    tp = len(parts)
    fs, height, cols = parts[0].shape
    matrix = (fs * height, tp * cols)
    out = (tp * rows[0].shape[0], tp * cols)
    return pl.pallas_call(
        functools.partial(gate_kernel, fs, tp),
        grid_spec=pltpu.PrefetchScalarGridSpec(
            num_scalar_prefetch=1,
            grid=(1,),
            in_specs=[whole(rows[0].shape)] * tp + [whole(parts[0].shape)] * tp,
            out_specs=[whole(matrix), whole(out)],
            scratch_shapes=[pltpu.VMEM((out[0], matrix[0]), bf16)],
        ),
        out_shape=[jax.ShapeDtypeStruct(matrix, bf16), jax.ShapeDtypeStruct(out, f32)],
        compiler_params=grant(24),
        cost_estimate=cost(2 * out[0] * matrix[0] * matrix[1], 4 * matrix[0] * matrix[1]),
    )(me, *rows, *parts)


def assemble(me_ref, parts, matrix_ref):
    fs, rows = len(parts), parts[0].shape[0]
    for r in range(fs):
        origin = lax.rem(me_ref[0] - r + fs, fs)
        matrix_ref[pl.ds(pl.multiple_of(origin * rows, rows), rows), :] = parts[r][...]


def up_kernel(fs, tp, me_ref, *refs):
    x_refs, parts, refs = refs[:tp], refs[tp : tp + fs], refs[tp + fs :]
    gate_ref, matrix_ref, out_ref, rows_ref = refs
    assemble(me_ref, parts, matrix_ref)
    up = product_of(x_refs, matrix_ref, rows_ref)
    gate = gate_ref[...]
    out_ref[...] = (gate / (1.0 + jnp.exp(-gate)) * up).astype(bf16)


def up_rows(me, rows, parts, gate):
    tp, fs = len(rows), len(parts)
    matrix = (fs * parts[0].shape[0], parts[0].shape[1])
    return pl.pallas_call(
        functools.partial(up_kernel, fs, tp),
        grid_spec=pltpu.PrefetchScalarGridSpec(
            num_scalar_prefetch=1,
            grid=(1,),
            in_specs=[whole(rows[0].shape)] * tp
            + [whole(parts[0].shape)] * fs
            + [whole(gate.shape)],
            out_specs=[whole(matrix), whole(gate.shape)],
            scratch_shapes=[pltpu.VMEM((gate.shape[0], matrix[0]), bf16)],
        ),
        out_shape=[jax.ShapeDtypeStruct(matrix, bf16), jax.ShapeDtypeStruct(gate.shape, bf16)],
        compiler_params=grant(24),
        cost_estimate=cost(2 * gate.size * matrix[0], 4 * matrix[0] * matrix[1]),
    )(me, *rows, *parts, gate)


def down_kernel(fs, tp, low, aliased, me_ref, hidden_ref, *refs):
    w_refs, refs = refs[:tp], refs[tp:]
    parts, refs = refs[:fs], refs[fs:]
    if aliased:
        refs = refs[1:]
    matrix_ref, outs, block, done = refs[0], refs[1 : 1 + tp], refs[1 + tp], refs[2 + tp]
    assemble(me_ref, parts, block)
    copy = pltpu.make_async_copy(block, matrix_ref.at[:, pl.ds(low, block.shape[1])], done)
    copy.start()
    product = jnp.dot(hidden_ref[...], block[...], preferred_element_type=f32)
    product = product.astype(bf16).astype(f32)
    count = w_refs[0].shape[0]
    lane = lax.broadcasted_iota(jnp.int32, (count, lanes), 1)
    mine = me_ref[1]
    chosen = (lane == mine) | (lane == mine + tp) | (lane == mine + 2 * tp)
    for q in range(tp):
        weight = jnp.sum(
            jnp.where(chosen, w_refs[q][...].astype(f32), 0.0), axis=1, keepdims=True
        )
        outs[q][...] = (product[q * count : (q + 1) * count] * weight).astype(bf16)
    copy.wait()


def down_rows(me, hidden, rows, parts, low, width, prior):
    tp, fs = len(rows), len(parts)
    count = rows[0].shape[0]
    depth = hidden.shape[1]
    size = parts[0].shape[1]
    weight_block = width // lanes
    in_specs = [whole(hidden.shape)]
    in_specs += [pl.BlockSpec((count, lanes), lambda k, m: (0, weight_block))] * tp
    in_specs += [whole(part.shape) for part in parts]
    args = [hidden, *rows, *parts]
    aliases = {}
    if prior is not None:
        in_specs.append(pl.BlockSpec(memory_space=pl.ANY))
        args.append(prior)
        aliases = {len(args): 0}
    outs = pl.pallas_call(
        functools.partial(down_kernel, fs, tp, low, prior is not None),
        grid_spec=pltpu.PrefetchScalarGridSpec(
            num_scalar_prefetch=1,
            grid=(1,),
            in_specs=in_specs,
            out_specs=[pl.BlockSpec(memory_space=pl.ANY)] + [whole((count, size))] * tp,
            scratch_shapes=[pltpu.VMEM((depth, size), bf16), pltpu.SemaphoreType.DMA],
        ),
        out_shape=[jax.ShapeDtypeStruct((depth, width), bf16)]
        + [jax.ShapeDtypeStruct((count, size), bf16)] * tp,
        input_output_aliases=aliases,
        compiler_params=grant(16),
        cost_estimate=cost(2 * tp * count * depth * size, 4 * depth * size),
    )(me, *args)
    return outs[0], outs[1:]


def final_kernel(fs, tp, me_ref, ids_ref, *refs):
    ins, out_ref = refs[:-1], refs[-1]
    onehot = slot_onehot(group_of(ids_ref[0:1, :], fs, tp), me_ref[0], fs)
    low = 0
    for ref in ins:
        back = jnp.concatenate([ref[lax.rem(me_ref[0] + r, fs)] for r in range(fs)], axis=0)
        high = low + back.shape[1]
        out_ref[:, low:high] = jnp.dot(onehot, back, preferred_element_type=f32).astype(bf16)
        low = high


def shards(tokens, norm_gain, gate_proj, up_proj, down_proj, expert_ids, route_weight):
    fs = lax.axis_size("fs")
    tp = lax.axis_size("tp")
    me = jnp.stack([lax.axis_index("fs"), lax.axis_index("tp")]).astype(jnp.int32)
    count, width = tokens.shape
    cuts = cuts_of(width)
    in_smem = pl.BlockSpec(memory_space=pltpu.SMEM)
    in_vmem = pl.BlockSpec(memory_space=pltpu.VMEM)

    def rotate(parts, axis, back=False, distances=None):
        n = len(parts)
        out = list(parts)
        for r in distances or far_first(n):
            step = n - r if back else r
            out[r] = lax.ppermute(parts[r], axis, [(k, (k + step) % n) for k in range(n)])
        return out

    def by_expert(matrix):
        return matrix.reshape((fs, tp) + matrix.shape[1:])

    ids, weights = expert_ids.T, route_weight.T
    scale = norm_gain[None, :]

    gate_parts = [None] * fs
    early, late = far_first(fs)[:3], far_first(fs)[3:]
    for k, distances in enumerate((early, late + [0])):
        cut = cast_along(me, by_expert(gate_proj), scale, 0, distances, None if k == 0 else grant(16))
        for r, part in zip(distances, cut):
            gate_parts[r] = part
        gate_parts = rotate(gate_parts, "fs", distances=[r for r in distances if r > 0])
    up_parts = cast_along(me, by_expert(up_proj), scale, 1, range(tp), grant(16))
    up_parts = rotate(up_parts, "tp")
    sent = pl.pallas_call(
        functools.partial(prep_kernel, fs, tp),
        in_specs=[in_smem, in_vmem, in_vmem, in_vmem],
        out_shape=[jax.ShapeDtypeStruct((count // fs, width + lanes), bf16)] * fs,
        compiler_params=grant(16),
        cost_estimate=cost(2 * count * count * width, 4 * count * width),
    )(me, tokens, ids, weights)
    landed = rotate(sent, "fs")
    down_parts = cast_along(me, by_expert(down_proj), None, 1, range(tp), grant(16))
    down_parts = rotate(down_parts, "tp")
    (up_parts,) = merge(me, up_parts, [(0, tp * up_parts[0].shape[2])])
    up_parts = rotate(up_parts, "fs")
    gate_parts = regroup(me, gate_parts)
    gate_parts = rotate(gate_parts, "tp")
    landed = join(landed)
    rows = rotate([landed] * tp, "tp")
    down_parts = merge(me, down_parts, cuts)
    for k in range(len(cuts)):
        down_parts[k] = rotate(down_parts[k], "fs")
    new_gate, gate = gate_rows(me, rows, gate_parts)
    new_up, hidden = up_rows(me, rows, up_parts, gate)
    new_down = None
    partials = []
    for k, (low, _) in enumerate(cuts):
        new_down, partial = down_rows(me, hidden, rows, down_parts[k], low, width, new_down)
        partials.append(rotate(partial, "tp", back=True))
    backs = []
    for members in returns:
        summed = add(me, fs, [partials[m] for m in members])
        backs.append(lax.all_to_all(summed, "fs", 0, 0, tiled=True))
    mixed = pl.pallas_call(
        functools.partial(final_kernel, fs, tp),
        in_specs=[in_smem] + [in_vmem] * (1 + len(backs)),
        out_shape=jax.ShapeDtypeStruct((count, width), bf16),
        compiler_params=grant(16),
        cost_estimate=cost(2 * count * count * width, 4 * count * width),
    )(me, ids, *backs)
    return (mixed, new_gate[None], new_up[None], new_down[None])


def solution(mesh):
    in_specs = (
        P(("fs", "tp"), None),
        P("fs"),
        P(None, "fs", "tp"),
        P(None, "fs", "tp"),
        P(None, "fs", "tp"),
        P(("fs", "tp"), None),
        P(("fs", "tp"), None),
    )
    out_specs = (
        P(("fs", "tp"), None),
        P(("fs", "tp"), None, None),
        P(("fs", "tp"), None, None),
        P(("fs", "tp"), None, None),
    )

    return jax.shard_map(shards, mesh=mesh, in_specs=in_specs, out_specs=out_specs, check_vma=False)
```

```python
import functools

import jax
import jax.numpy as jnp
from jax import lax
from jax.experimental import pallas as pl
from jax.experimental.pallas import tpu as pltpu
from jax.sharding import PartitionSpec as P


norm_eps = 1e-06
lanes = 128
bf16 = jnp.bfloat16
f32 = jnp.float32


def cuts_of(width):
    half, rest = width // 2, width - width // 8
    return [(0, half), (half, rest), (rest, width)]


returns = [(0,), (1, 2)]


def grant(mib):
    return pltpu.CompilerParams(vmem_limit_bytes=mib * 1024 * 1024)


def far_first(n):
    return sorted(range(1, n), key=lambda r: (abs(2 * r - n), r))


def cost(flops, nbytes):
    return pl.CostEstimate(flops=int(flops), bytes_accessed=int(nbytes), transcendentals=0)


def whole(shape):
    return pl.BlockSpec(shape, lambda *_: (0,) * len(shape))


def square(n):
    return lax.broadcasted_iota(jnp.int32, (n, n), 0), lax.broadcasted_iota(jnp.int32, (n, n), 1)


def to_col(row):
    n = row.shape[1]
    down, across = square(n)
    return jnp.sum(jnp.where(down == across, row, jnp.zeros((), row.dtype)), axis=1, keepdims=True)


def slot_onehot(group_row, fs):
    count = group_row.shape[1]
    down, across = square(count)
    group_col = to_col(group_row)
    earlier = jnp.where((group_col == group_row) & (across < down), 1.0, 0.0)
    rank = jnp.sum(earlier, axis=1, keepdims=True)
    slot = (group_col * float(count // fs) + rank).astype(jnp.int32)
    return jnp.where(slot == across, 1.0, 0.0).astype(bf16)


def group_of(ids, fs, tp):
    group = jnp.zeros(ids.shape, f32)
    for bound in range(1, fs):
        group = group + jnp.where(ids >= bound * tp, 1.0, 0.0)
    return group


def prep_kernel(fs, tp, tok_ref, ids_ref, weight_ref, out_ref):
    count, width = tok_ref.shape
    group = group_of(ids_ref[0:1, :], fs, tp)
    onehot = slot_onehot(group, fs)
    wide = tok_ref[...].astype(f32)
    scale = lax.rsqrt(jnp.mean(wide * wide, axis=-1, keepdims=True) + norm_eps)
    normed = (wide * scale).astype(bf16)
    lane = lax.broadcasted_iota(jnp.int32, (count, lanes), 1)
    extra = jnp.zeros((count, lanes), f32)
    for pick in range(2):
        local = ids_ref[pick : pick + 1, :].astype(f32) - group * float(tp)
        local = to_col(local).astype(jnp.int32)
        rest = to_col(weight_ref[pick : pick + 1, :])
        for part in range(3):
            piece = rest.astype(bf16).astype(f32)
            extra = extra + jnp.where(lane == local + part * tp, piece, 0.0)
            rest = rest - piece
    dims = (((0,), (0,)), ((), ()))
    rows = lax.dot_general(onehot, normed, dims, preferred_element_type=f32).astype(bf16)
    extra = lax.dot_general(onehot, extra.astype(bf16), dims, preferred_element_type=f32).astype(bf16)
    out_ref[:, :width] = rows
    out_ref[:, width:] = extra


def add_kernel(tp, *refs):
    ins, out_ref = refs[:-1], refs[-1]
    fs, each, _ = out_ref.shape
    low = 0
    for k in range(0, len(ins), tp):
        total = sum(ref[...].astype(f32) for ref in ins[k : k + tp]).astype(bf16)
        high = low + total.shape[1]
        for r in range(fs):
            out_ref[r, :, low:high] = total[r * each : (r + 1) * each]
        low = high


def add(fs, groups):
    tp = len(groups[0])
    count = groups[0][0].shape[0]
    width = sum(group[0].shape[1] for group in groups)
    terms = [part for group in groups for part in group]
    return pl.pallas_call(
        functools.partial(add_kernel, tp),
        out_shape=jax.ShapeDtypeStruct((fs, count // fs, width), bf16),
        compiler_params=grant(8),
        cost_estimate=cost(1e9, 2 * (tp + 1) * count * width),
    )(*terms)


def cast_kernel(steps, scaled, squeeze, me_ref, in_ref, *refs):
    step = pl.program_id(0)
    value = in_ref[:, 0] if squeeze else in_ref[0]
    if scaled:
        value = value * to_col(refs[0][...])[None]
        refs = refs[1:]
    value = value.astype(bf16)
    for k in range(steps):

        @pl.when(step == k)
        def _(k=k):
            refs[k][...] = value


def cast_along(me, matrix, scale, axis, distances, params):
    fs, tp, rows, cols = matrix.shape
    steps = len(distances)

    def target(k, m):
        ahead = jnp.int32(distances[0])
        for j in range(1, steps):
            ahead = jnp.where(k == j, jnp.int32(distances[j]), ahead)
        return lax.rem(m[axis] + ahead, (fs, tp)[axis])

    if axis == 0:
        in_spec = pl.BlockSpec((1, tp, rows, cols), lambda k, m: (target(k, m), 0, 0, 0))
        shape = (tp, rows, cols)
    else:
        in_spec = pl.BlockSpec((fs, 1, rows, cols), lambda k, m: (0, target(k, m), 0, 0))
        shape = (fs, rows, cols)
    in_specs, args = [in_spec], [matrix]
    if scale is not None:
        in_specs.append(whole(scale.shape))
        args.append(scale)
    return pl.pallas_call(
        functools.partial(cast_kernel, steps, scale is not None, axis == 1),
        grid_spec=pltpu.PrefetchScalarGridSpec(
            num_scalar_prefetch=1, grid=(steps,), in_specs=in_specs, out_specs=[whole(shape)] * steps
        ),
        out_shape=[jax.ShapeDtypeStruct(shape, bf16)] * steps,
        compiler_params=params,
        cost_estimate=cost(1e9, 6 * matrix.size * steps // (fs, tp)[axis]),
    )(me, *args)


def in_order(me_ref, tp, action):
    for value in range(tp):

        @pl.when(me_ref[1] == value)
        def _(value=value):
            action([(value - j) % tp for j in range(tp)])


def merge_kernel(fs, tp, cuts, me_ref, *refs):
    ins, outs = refs[:tp], refs[tp:]

    def store(order):
        for r in range(fs):
            group = lax.rem(me_ref[0] + r, fs)
            full = jnp.concatenate([ins[q][group] for q in order], axis=-1)
            for k, (low, high) in enumerate(cuts):
                outs[k * fs + r][...] = full[:, low:high]

    in_order(me_ref, tp, store)


def merge(me, parts, cuts):
    tp = len(parts)
    fs, rows, _ = parts[0].shape
    shapes = [(rows, high - low) for low, high in cuts for _ in range(fs)]
    outs = pl.pallas_call(
        functools.partial(merge_kernel, fs, tp, cuts),
        grid_spec=pltpu.PrefetchScalarGridSpec(
            num_scalar_prefetch=1,
            grid=(1,),
            in_specs=[whole(parts[0].shape)] * tp,
            out_specs=[whole(shape) for shape in shapes],
        ),
        out_shape=[jax.ShapeDtypeStruct(shape, bf16) for shape in shapes],
        compiler_params=grant(16),
        cost_estimate=cost(1e9, 4 * tp * parts[0].size),
    )(me, *parts)
    return [outs[k * fs : (k + 1) * fs] for k in range(len(cuts))]


def regroup_kernel(fs, tp, me_ref, *refs):
    for q in range(tp):
        target = lax.rem(me_ref[1] + q, tp)
        for r in range(fs):
            refs[fs + q][r] = refs[r][target]


def regroup(me, parts):
    fs = len(parts)
    tp, rows, cols = parts[0].shape
    shape = (fs, rows, cols)
    return pl.pallas_call(
        functools.partial(regroup_kernel, fs, tp),
        grid_spec=pltpu.PrefetchScalarGridSpec(
            num_scalar_prefetch=1,
            grid=(1,),
            in_specs=[whole(parts[0].shape)] * fs,
            out_specs=[whole(shape)] * tp,
        ),
        out_shape=[jax.ShapeDtypeStruct(shape, bf16)] * tp,
        compiler_params=grant(16),
        cost_estimate=cost(1e9, 4 * fs * parts[0].size),
    )(me, *parts)


def product_of(x_refs, matrix_ref, rows_ref):
    width = matrix_ref.shape[0]
    count = x_refs[0].shape[0]
    for q, ref in enumerate(x_refs):
        rows_ref[q * count : (q + 1) * count, :] = ref[:, :width]
    return jnp.dot(rows_ref[...], matrix_ref[...], preferred_element_type=f32)


def gate_kernel(fs, tp, me_ref, *refs):
    x_refs, parts, (matrix_ref, out_ref, rows_ref) = refs[:tp], refs[tp : 2 * tp], refs[2 * tp :]
    height = parts[0].shape[1]

    def store(order):
        for r in range(fs):
            origin = lax.rem(me_ref[0] - r + fs, fs)
            matrix_ref[pl.ds(pl.multiple_of(origin * height, height), height), :] = jnp.concatenate(
                [parts[q][r] for q in order], axis=-1
            )

    in_order(me_ref, tp, store)
    out_ref[...] = product_of(x_refs, matrix_ref, rows_ref)


def gate_rows(me, rows, parts):
    tp = len(parts)
    fs, height, cols = parts[0].shape
    matrix = (fs * height, tp * cols)
    out = (tp * rows[0].shape[0], tp * cols)
    return pl.pallas_call(
        functools.partial(gate_kernel, fs, tp),
        grid_spec=pltpu.PrefetchScalarGridSpec(
            num_scalar_prefetch=1,
            grid=(1,),
            in_specs=[whole(rows[0].shape)] * tp + [whole(parts[0].shape)] * tp,
            out_specs=[whole(matrix), whole(out)],
            scratch_shapes=[pltpu.VMEM((out[0], matrix[0]), bf16)],
        ),
        out_shape=[jax.ShapeDtypeStruct(matrix, bf16), jax.ShapeDtypeStruct(out, f32)],
        compiler_params=grant(24),
        cost_estimate=cost(2 * out[0] * matrix[0] * matrix[1], 4 * matrix[0] * matrix[1]),
    )(me, *rows, *parts)


def assemble(me_ref, parts, matrix_ref):
    fs, rows = len(parts), parts[0].shape[0]
    for r in range(fs):
        origin = lax.rem(me_ref[0] - r + fs, fs)
        matrix_ref[pl.ds(pl.multiple_of(origin * rows, rows), rows), :] = parts[r][...]


def up_kernel(fs, tp, me_ref, *refs):
    x_refs, parts, refs = refs[:tp], refs[tp : tp + fs], refs[tp + fs :]
    gate_ref, matrix_ref, out_ref, rows_ref = refs
    assemble(me_ref, parts, matrix_ref)
    up = product_of(x_refs, matrix_ref, rows_ref)
    gate = gate_ref[...]
    out_ref[...] = (gate / (1.0 + jnp.exp(-gate)) * up).astype(bf16)


def up_rows(me, rows, parts, gate):
    tp, fs = len(rows), len(parts)
    matrix = (fs * parts[0].shape[0], parts[0].shape[1])
    return pl.pallas_call(
        functools.partial(up_kernel, fs, tp),
        grid_spec=pltpu.PrefetchScalarGridSpec(
            num_scalar_prefetch=1,
            grid=(1,),
            in_specs=[whole(rows[0].shape)] * tp
            + [whole(parts[0].shape)] * fs
            + [whole(gate.shape)],
            out_specs=[whole(matrix), whole(gate.shape)],
            scratch_shapes=[pltpu.VMEM((gate.shape[0], matrix[0]), bf16)],
        ),
        out_shape=[jax.ShapeDtypeStruct(matrix, bf16), jax.ShapeDtypeStruct(gate.shape, bf16)],
        compiler_params=grant(24),
        cost_estimate=cost(2 * gate.size * matrix[0], 4 * matrix[0] * matrix[1]),
    )(me, *rows, *parts, gate)


def down_kernel(fs, tp, low, aliased, me_ref, hidden_ref, *refs):
    w_refs, refs = refs[:tp], refs[tp:]
    parts, refs = refs[:fs], refs[fs:]
    if aliased:
        refs = refs[1:]
    matrix_ref, outs, block, done = refs[0], refs[1 : 1 + tp], refs[1 + tp], refs[2 + tp]
    assemble(me_ref, parts, block)
    copy = pltpu.make_async_copy(block, matrix_ref.at[:, pl.ds(low, block.shape[1])], done)
    copy.start()
    product = jnp.dot(hidden_ref[...], block[...], preferred_element_type=f32)
    product = product.astype(bf16).astype(f32)
    count = w_refs[0].shape[0]
    lane = lax.broadcasted_iota(jnp.int32, (count, lanes), 1)
    mine = me_ref[1]
    chosen = (lane == mine) | (lane == mine + tp) | (lane == mine + 2 * tp)
    for q in range(tp):
        weight = jnp.sum(
            jnp.where(chosen, w_refs[q][...].astype(f32), 0.0), axis=1, keepdims=True
        )
        outs[q][...] = (product[q * count : (q + 1) * count] * weight).astype(bf16)
    copy.wait()


def down_rows(me, hidden, rows, parts, low, width, prior):
    tp, fs = len(rows), len(parts)
    count = rows[0].shape[0]
    depth = hidden.shape[1]
    size = parts[0].shape[1]
    weight_block = width // lanes
    in_specs = [whole(hidden.shape)]
    in_specs += [pl.BlockSpec((count, lanes), lambda k, m: (0, weight_block))] * tp
    in_specs += [whole(part.shape) for part in parts]
    args = [hidden, *rows, *parts]
    aliases = {}
    if prior is not None:
        in_specs.append(pl.BlockSpec(memory_space=pl.ANY))
        args.append(prior)
        aliases = {len(args): 0}
    outs = pl.pallas_call(
        functools.partial(down_kernel, fs, tp, low, prior is not None),
        grid_spec=pltpu.PrefetchScalarGridSpec(
            num_scalar_prefetch=1,
            grid=(1,),
            in_specs=in_specs,
            out_specs=[pl.BlockSpec(memory_space=pl.ANY)] + [whole((count, size))] * tp,
            scratch_shapes=[pltpu.VMEM((depth, size), bf16), pltpu.SemaphoreType.DMA],
        ),
        out_shape=[jax.ShapeDtypeStruct((depth, width), bf16)]
        + [jax.ShapeDtypeStruct((count, size), bf16)] * tp,
        input_output_aliases=aliases,
        compiler_params=grant(16),
        cost_estimate=cost(2 * tp * count * depth * size, 4 * depth * size),
    )(me, *args)
    return outs[0], outs[1:]


def final_kernel(fs, tp, ids_ref, *refs):
    ins, out_ref = refs[:-1], refs[-1]
    onehot = slot_onehot(group_of(ids_ref[0:1, :], fs, tp), fs)
    low = 0
    for ref in ins:
        back = jnp.concatenate([ref[g] for g in range(fs)], axis=0)
        high = low + back.shape[1]
        out_ref[:, low:high] = jnp.dot(onehot, back, preferred_element_type=f32).astype(bf16)
        low = high


def shards(tokens, norm_gain, gate_proj, up_proj, down_proj, expert_ids, route_weight):
    fs = lax.axis_size("fs")
    tp = lax.axis_size("tp")
    me = jnp.stack([lax.axis_index("fs"), lax.axis_index("tp")]).astype(jnp.int32)
    count, width = tokens.shape
    cuts = cuts_of(width)

    def rotate(parts, axis, distances=None):
        n = len(parts)
        out = list(parts)
        for r in distances or far_first(n):
            out[r] = lax.ppermute(parts[r], axis, [(k, (k + r) % n) for k in range(n)])
        return out

    def by_expert(matrix):
        return matrix.reshape((fs, tp) + matrix.shape[1:])

    ids, weights = expert_ids.T, route_weight.T
    scale = norm_gain[None, :]

    sent = pl.pallas_call(
        functools.partial(prep_kernel, fs, tp),
        out_shape=jax.ShapeDtypeStruct((count, width + lanes), bf16),
        cost_estimate=cost(2 * count * count * width, 4 * count * width),
    )(tokens, ids, weights)
    landed = lax.all_to_all(sent.reshape(fs, count // fs, -1), "fs", 0, 0, tiled=True)
    landed = landed.reshape(count, -1)
    gate_parts = [None] * fs
    early, late = far_first(fs)[:3], far_first(fs)[3:]

    def cut_gate(distances, params):
        cut = cast_along(me, by_expert(gate_proj), scale, 0, distances, params)
        for r, part in zip(distances, cut):
            gate_parts[r] = part
        gate_parts[:] = rotate(gate_parts, "fs", distances=[r for r in distances if r > 0])

    cut_gate(early, None)
    up_parts = cast_along(me, by_expert(up_proj), scale, 1, range(tp), grant(16))
    up_parts = rotate(up_parts, "tp")
    cut_gate(late + [0], grant(16))
    down_parts = cast_along(me, by_expert(down_proj), None, 1, range(tp), grant(16))
    down_parts = rotate(down_parts, "tp")
    source = [
        [((j ^ core) - step) % tp for j in range(tp)] for core in (0, 1) for step in range(0, tp, 2)
    ]
    rows = [landed] + [
        lax.ppermute(landed, "tp", [(k, (k + step) % tp) for k in range(tp)])
        for step in range(2, tp, 2)
    ]
    rows += [lax.ppermute(part, "tp", [(k, k ^ 1) for k in range(tp)]) for part in rows]
    (up_parts,) = merge(me, up_parts, [(0, tp * up_parts[0].shape[2])])
    for distances in (early, late):
        up_parts = rotate(up_parts, "fs", distances)
    gate_parts = regroup(me, gate_parts)
    gate_parts = rotate(gate_parts, "tp")
    down_parts = merge(me, down_parts, cuts)
    for k in range(len(cuts)):
        down_parts[k] = rotate(down_parts[k], "fs")
    new_gate, gate = gate_rows(me, rows, gate_parts)
    new_up, hidden = up_rows(me, rows, up_parts, gate)
    new_down = None
    partials = []
    for k, (low, _) in enumerate(cuts):
        new_down, partial = down_rows(me, hidden, rows, down_parts[k], low, width, new_down)
        partials.append(
            [partial[0]]
            + [
                lax.ppermute(term, "tp", list(enumerate(places)))
                for term, places in zip(partial[1:], source[1:])
            ]
        )
    backs = []
    for members in returns:
        summed = add(fs, [partials[m] for m in members])
        backs.append(lax.all_to_all(summed, "fs", 0, 0, tiled=True))
    mixed = pl.pallas_call(
        functools.partial(final_kernel, fs, tp),
        out_shape=jax.ShapeDtypeStruct((count, width), bf16),
        compiler_params=grant(16),
        cost_estimate=cost(2 * count * count * width, 4 * count * width),
    )(ids, *backs)
    return (mixed, new_gate[None], new_up[None], new_down[None])


def solution(mesh):
    in_specs = (
        P(("fs", "tp"), None),
        P("fs"),
        P(None, "fs", "tp"),
        P(None, "fs", "tp"),
        P(None, "fs", "tp"),
        P(("fs", "tp"), None),
        P(("fs", "tp"), None),
    )
    out_specs = (
        P(("fs", "tp"), None),
        P(("fs", "tp"), None, None),
        P(("fs", "tp"), None, None),
        P(("fs", "tp"), None, None),
    )

    return jax.shard_map(shards, mesh=mesh, in_specs=in_specs, out_specs=out_specs, check_vma=False)
```

```python
import functools

import jax
import jax.numpy as jnp
from jax import lax
from jax.experimental import pallas as pl
from jax.experimental.pallas import tpu as pltpu
from jax.sharding import PartitionSpec as P


norm_eps = 1e-06
lanes = 128
bf16 = jnp.bfloat16
f32 = jnp.float32


def cuts_of(width):
    first = width // 8 * 5
    return [(0, first), (first, width)]


def grant(mib):
    return pltpu.CompilerParams(vmem_limit_bytes=mib * 1024 * 1024)


def far_first(n):
    return sorted(range(1, n), key=lambda r: (abs(2 * r - n), r))


def cost(flops, nbytes):
    return pl.CostEstimate(flops=int(flops), bytes_accessed=int(nbytes), transcendentals=0)


def whole(shape):
    return pl.BlockSpec(shape, lambda *_: (0,) * len(shape))


def square(n):
    return lax.broadcasted_iota(jnp.int32, (n, n), 0), lax.broadcasted_iota(jnp.int32, (n, n), 1)


def to_col(row):
    n = row.shape[1]
    down, across = square(n)
    return jnp.sum(jnp.where(down == across, row, jnp.zeros((), row.dtype)), axis=1, keepdims=True)


def slot_onehot(group_row, fs):
    count = group_row.shape[1]
    down, across = square(count)
    group_col = to_col(group_row)
    earlier = jnp.where((group_col == group_row) & (across < down), 1.0, 0.0)
    rank = jnp.sum(earlier, axis=1, keepdims=True)
    slot = (group_col * float(count // fs) + rank).astype(jnp.int32)
    return jnp.where(slot == across, 1.0, 0.0).astype(bf16)


def group_of(ids, fs, tp):
    group = jnp.zeros(ids.shape, f32)
    for bound in range(1, fs):
        group = group + jnp.where(ids >= bound * tp, 1.0, 0.0)
    return group


def prep_kernel(fs, tp, tok_ref, ids_ref, weight_ref, out_ref):
    count, width = tok_ref.shape
    group = group_of(ids_ref[0:1, :], fs, tp)
    onehot = slot_onehot(group, fs)
    wide = tok_ref[...].astype(f32)
    scale = lax.rsqrt(jnp.mean(wide * wide, axis=-1, keepdims=True) + norm_eps)
    normed = (wide * scale).astype(bf16)
    lane = lax.broadcasted_iota(jnp.int32, (count, lanes), 1)
    extra = jnp.zeros((count, lanes), f32)
    for pick in range(2):
        local = ids_ref[pick : pick + 1, :].astype(f32) - group * float(tp)
        local = to_col(local).astype(jnp.int32)
        rest = to_col(weight_ref[pick : pick + 1, :])
        for part in range(3):
            piece = rest.astype(bf16).astype(f32)
            extra = extra + jnp.where(lane == local + part * tp, piece, 0.0)
            rest = rest - piece
    dims = (((0,), (0,)), ((), ()))
    rows = lax.dot_general(onehot, normed, dims, preferred_element_type=f32).astype(bf16)
    extra = lax.dot_general(onehot, extra.astype(bf16), dims, preferred_element_type=f32).astype(bf16)
    out_ref[:, :width] = rows
    out_ref[:, width:] = extra


def add_kernel(*refs):
    out_ref = refs[-1]
    fs, each, _ = out_ref.shape
    total = sum(ref[...].astype(f32) for ref in refs[:-1]).astype(bf16)
    for i in range(fs):
        out_ref[i] = total[i * each : (i + 1) * each]


def add(fs, terms):
    count, width = terms[0].shape
    return pl.pallas_call(
        add_kernel,
        out_shape=jax.ShapeDtypeStruct((fs, count // fs, width), bf16),
        compiler_params=grant(8),
        cost_estimate=cost(1e9, 2 * (len(terms) + 1) * count * width),
    )(*terms)


def cast_kernel(steps, scaled, squeeze, me_ref, in_ref, *refs):
    step = pl.program_id(0)
    value = in_ref[:, 0] if squeeze else in_ref[0]
    if scaled:
        value = value * to_col(refs[0][...])[None]
        refs = refs[1:]
    value = value.astype(bf16)
    for k in range(steps):

        @pl.when(step == k)
        def _(k=k):
            refs[k][...] = value


def cast_along(me, matrix, scale, axis, distances, params):
    fs, tp, rows, cols = matrix.shape
    steps = len(distances)

    def target(k, m):
        ahead = jnp.int32(distances[0])
        for j in range(1, steps):
            ahead = jnp.where(k == j, jnp.int32(distances[j]), ahead)
        return lax.rem(m[axis] + ahead, (fs, tp)[axis])

    if axis == 0:
        in_spec = pl.BlockSpec((1, tp, rows, cols), lambda k, m: (target(k, m), 0, 0, 0))
        shape = (tp, rows, cols)
    else:
        in_spec = pl.BlockSpec((fs, 1, rows, cols), lambda k, m: (0, target(k, m), 0, 0))
        shape = (fs, rows, cols)
    in_specs, args = [in_spec], [matrix]
    if scale is not None:
        in_specs.append(whole(scale.shape))
        args.append(scale)
    return pl.pallas_call(
        functools.partial(cast_kernel, steps, scale is not None, axis == 1),
        grid_spec=pltpu.PrefetchScalarGridSpec(
            num_scalar_prefetch=1, grid=(steps,), in_specs=in_specs, out_specs=[whole(shape)] * steps
        ),
        out_shape=[jax.ShapeDtypeStruct(shape, bf16)] * steps,
        compiler_params=params,
        cost_estimate=cost(1e9, 6 * matrix.size * steps // (fs, tp)[axis]),
    )(me, *args)


def in_order(me_ref, tp, action):
    for value in range(tp):

        @pl.when(me_ref[1] == value)
        def _(value=value):
            action([(value - j) % tp for j in range(tp)])


def merge_kernel(fs, tp, cuts, me_ref, *refs):
    ins, outs = refs[:tp], refs[tp:]

    def store(order):
        for r in range(fs):
            group = lax.rem(me_ref[0] + r, fs)
            full = jnp.concatenate([ins[q][group] for q in order], axis=-1)
            for k, (low, high) in enumerate(cuts[:-1]):
                outs[k * fs + r][...] = full[:, low:high]
            outs[-1][group] = full[:, cuts[-1][0] :]

    in_order(me_ref, tp, store)


def merge(me, parts, cuts):
    tp = len(parts)
    fs, rows, _ = parts[0].shape
    shapes = [(rows, high - low) for low, high in cuts[:-1] for _ in range(fs)]
    shapes.append((fs, rows, cuts[-1][1] - cuts[-1][0]))
    outs = pl.pallas_call(
        functools.partial(merge_kernel, fs, tp, cuts),
        grid_spec=pltpu.PrefetchScalarGridSpec(
            num_scalar_prefetch=1,
            grid=(1,),
            in_specs=[whole(parts[0].shape)] * tp,
            out_specs=[whole(shape) for shape in shapes],
        ),
        out_shape=[jax.ShapeDtypeStruct(shape, bf16) for shape in shapes],
        compiler_params=grant(16),
        cost_estimate=cost(1e9, 4 * tp * parts[0].size),
    )(me, *parts)
    return [outs[k * fs : (k + 1) * fs] for k in range(len(cuts) - 1)] + [outs[-1]]


def regroup_kernel(fs, tp, me_ref, *refs):
    for q in range(tp):
        target = lax.rem(me_ref[1] + q, tp)
        for r in range(fs):
            refs[fs + q][r] = refs[r][target]


def regroup(me, parts):
    fs = len(parts)
    tp, rows, cols = parts[0].shape
    shape = (fs, rows, cols)
    return pl.pallas_call(
        functools.partial(regroup_kernel, fs, tp),
        grid_spec=pltpu.PrefetchScalarGridSpec(
            num_scalar_prefetch=1,
            grid=(1,),
            in_specs=[whole(parts[0].shape)] * fs,
            out_specs=[whole(shape)] * tp,
        ),
        out_shape=[jax.ShapeDtypeStruct(shape, bf16)] * tp,
        compiler_params=grant(16),
        cost_estimate=cost(1e9, 4 * fs * parts[0].size),
    )(me, *parts)


def product_of(x_refs, matrix_ref, rows_ref):
    width = matrix_ref.shape[0]
    count = x_refs[0].shape[0]
    for q, ref in enumerate(x_refs):
        rows_ref[q * count : (q + 1) * count, :] = ref[:, :width]
    return jnp.dot(rows_ref[...], matrix_ref[...], preferred_element_type=f32)


def gate_kernel(fs, tp, me_ref, *refs):
    x_refs, parts, (matrix_ref, out_ref, rows_ref) = refs[:tp], refs[tp : 2 * tp], refs[2 * tp :]
    height = parts[0].shape[1]

    def store(order):
        for r in range(fs):
            origin = lax.rem(me_ref[0] - r + fs, fs)
            matrix_ref[pl.ds(pl.multiple_of(origin * height, height), height), :] = jnp.concatenate(
                [parts[q][r] for q in order], axis=-1
            )

    in_order(me_ref, tp, store)
    out_ref[...] = product_of(x_refs, matrix_ref, rows_ref)


def gate_rows(me, rows, parts):
    tp = len(parts)
    fs, height, cols = parts[0].shape
    matrix = (fs * height, tp * cols)
    out = (tp * rows[0].shape[0], tp * cols)
    return pl.pallas_call(
        functools.partial(gate_kernel, fs, tp),
        grid_spec=pltpu.PrefetchScalarGridSpec(
            num_scalar_prefetch=1,
            grid=(1,),
            in_specs=[whole(rows[0].shape)] * tp + [whole(parts[0].shape)] * tp,
            out_specs=[whole(matrix), whole(out)],
            scratch_shapes=[pltpu.VMEM((out[0], matrix[0]), bf16)],
        ),
        out_shape=[jax.ShapeDtypeStruct(matrix, bf16), jax.ShapeDtypeStruct(out, f32)],
        compiler_params=grant(24),
        cost_estimate=cost(2 * out[0] * matrix[0] * matrix[1], 4 * matrix[0] * matrix[1]),
    )(me, *rows, *parts)


def assemble(me_ref, parts, matrix_ref):
    fs, rows = len(parts), parts[0].shape[0]
    if fs == 1:
        matrix_ref[...] = parts[0][...]
        return
    for r in range(fs):
        origin = lax.rem(me_ref[0] - r + fs, fs)
        matrix_ref[pl.ds(pl.multiple_of(origin * rows, rows), rows), :] = parts[r][...]


def up_kernel(tp, me_ref, *refs):
    x_refs, parts, refs = refs[:tp], refs[tp:-4], refs[-4:]
    gate_ref, matrix_ref, out_ref, rows_ref = refs
    assemble(me_ref, parts, matrix_ref)
    up = product_of(x_refs, matrix_ref, rows_ref)
    gate = gate_ref[...]
    out_ref[...] = (gate / (1.0 + jnp.exp(-gate)) * up).astype(bf16)


def up_rows(me, rows, parts, gate):
    tp = len(rows)
    matrix = (len(parts) * parts[0].shape[0], parts[0].shape[1])
    return pl.pallas_call(
        functools.partial(up_kernel, tp),
        grid_spec=pltpu.PrefetchScalarGridSpec(
            num_scalar_prefetch=1,
            grid=(1,),
            in_specs=[whole(rows[0].shape)] * tp
            + [whole(part.shape) for part in parts]
            + [whole(gate.shape)],
            out_specs=[whole(matrix), whole(gate.shape)],
            scratch_shapes=[pltpu.VMEM((gate.shape[0], matrix[0]), bf16)],
        ),
        out_shape=[jax.ShapeDtypeStruct(matrix, bf16), jax.ShapeDtypeStruct(gate.shape, bf16)],
        compiler_params=grant(24),
        cost_estimate=cost(2 * gate.size * matrix[0], 4 * matrix[0] * matrix[1]),
    )(me, *rows, *parts, gate)


def down_kernel(count_parts, tp, low, aliased, me_ref, hidden_ref, *refs):
    w_refs, refs = refs[:tp], refs[tp:]
    parts, refs = refs[:count_parts], refs[count_parts:]
    if aliased:
        refs = refs[1:]
    matrix_ref, outs, block, done = refs[0], refs[1 : 1 + tp], refs[1 + tp], refs[2 + tp]
    assemble(me_ref, parts, block)
    copy = pltpu.make_async_copy(block, matrix_ref.at[:, pl.ds(low, block.shape[1])], done)
    copy.start()
    product = jnp.dot(hidden_ref[...], block[...], preferred_element_type=f32)
    product = product.astype(bf16).astype(f32)
    count = w_refs[0].shape[0]
    lane = lax.broadcasted_iota(jnp.int32, (count, lanes), 1)
    mine = me_ref[1]
    chosen = (lane == mine) | (lane == mine + tp) | (lane == mine + 2 * tp)
    for q in range(tp):
        weight = jnp.sum(
            jnp.where(chosen, w_refs[q][...].astype(f32), 0.0), axis=1, keepdims=True
        )
        outs[q][...] = (product[q * count : (q + 1) * count] * weight).astype(bf16)
    copy.wait()


def down_rows(me, hidden, rows, parts, low, width, prior):
    tp = len(rows)
    count = rows[0].shape[0]
    depth = hidden.shape[1]
    size = parts[0].shape[1]
    weight_block = width // lanes
    in_specs = [whole(hidden.shape)]
    in_specs += [pl.BlockSpec((count, lanes), lambda k, m: (0, weight_block))] * tp
    in_specs += [whole(part.shape) for part in parts]
    args = [hidden, *rows, *parts]
    aliases = {}
    if prior is not None:
        in_specs.append(pl.BlockSpec(memory_space=pl.ANY))
        args.append(prior)
        aliases = {len(args): 0}
    outs = pl.pallas_call(
        functools.partial(down_kernel, len(parts), tp, low, prior is not None),
        grid_spec=pltpu.PrefetchScalarGridSpec(
            num_scalar_prefetch=1,
            grid=(1,),
            in_specs=in_specs,
            out_specs=[pl.BlockSpec(memory_space=pl.ANY)] + [whole((count, size))] * tp,
            scratch_shapes=[pltpu.VMEM((depth, size), bf16), pltpu.SemaphoreType.DMA],
        ),
        out_shape=[jax.ShapeDtypeStruct((depth, width), bf16)]
        + [jax.ShapeDtypeStruct((count, size), bf16)] * tp,
        input_output_aliases=aliases,
        compiler_params=grant(16),
        cost_estimate=cost(2 * tp * count * depth * size, 4 * depth * size),
    )(me, *args)
    return outs[0], outs[1:]


def final_kernel(fs, tp, ids_ref, *refs):
    ins, out_ref = refs[:-1], refs[-1]
    onehot = slot_onehot(group_of(ids_ref[0:1, :], fs, tp), fs)
    low = 0
    for ref in ins:
        high = low + ref.shape[1]
        out_ref[:, low:high] = jnp.dot(onehot, ref[...], preferred_element_type=f32).astype(bf16)
        low = high


def shards(tokens, norm_gain, gate_proj, up_proj, down_proj, expert_ids, route_weight):
    fs = lax.axis_size("fs")
    tp = lax.axis_size("tp")
    me = jnp.stack([lax.axis_index("fs"), lax.axis_index("tp")]).astype(jnp.int32)
    count, width = tokens.shape
    cuts = cuts_of(width)

    def rotate(parts, axis, distances=None):
        n = len(parts)
        out = list(parts)
        for r in distances or far_first(n):
            out[r] = lax.ppermute(parts[r], axis, [(k, (k + r) % n) for k in range(n)])
        return out

    def swap_fs(value):
        out = lax.all_to_all(value, "fs", 0, 0, tiled=True)
        return out.reshape(-1, out.shape[2])

    def by_expert(matrix):
        return matrix.reshape((fs, tp) + matrix.shape[1:])

    ids, weights = expert_ids.T, route_weight.T
    scale = norm_gain[None, :]

    sent = pl.pallas_call(
        functools.partial(prep_kernel, fs, tp),
        out_shape=jax.ShapeDtypeStruct((count, width + lanes), bf16),
        cost_estimate=cost(2 * count * count * width, 4 * count * width),
    )(tokens, ids, weights)
    landed = swap_fs(sent.reshape(fs, count // fs, -1))
    gate_parts = [None] * fs
    early, late = far_first(fs)[:3], far_first(fs)[3:]

    def cut_gate(distances, params):
        cut = cast_along(me, by_expert(gate_proj), scale, 0, distances, params)
        for r, part in zip(distances, cut):
            gate_parts[r] = part
        gate_parts[:] = rotate(gate_parts, "fs", distances=[r for r in distances if r > 0])

    cut_gate(early, None)
    up_parts = cast_along(me, by_expert(up_proj), scale, 1, range(tp), grant(16))
    up_parts = rotate(up_parts, "tp")
    cut_gate(late + [0], grant(16))
    down_parts = cast_along(me, by_expert(down_proj), None, 1, range(tp), grant(16))
    down_parts = rotate(down_parts, "tp")
    source = [
        [((j ^ core) - step) % tp for j in range(tp)] for core in (0, 1) for step in range(0, tp, 2)
    ]
    rows = [landed] + [
        lax.ppermute(landed, "tp", [(k, (k + step) % tp) for k in range(tp)])
        for step in range(2, tp, 2)
    ]
    rows += [lax.ppermute(part, "tp", [(k, k ^ 1) for k in range(tp)]) for part in rows]
    (up_here,) = merge(me, up_parts, [(0, tp * up_parts[0].shape[2])])
    up_parts = [swap_fs(up_here)]
    gate_parts = regroup(me, gate_parts)
    gate_parts = rotate(gate_parts, "tp")
    down_parts = merge(me, down_parts, cuts)
    new_gate, gate = gate_rows(me, rows, gate_parts)
    down_parts[0] = rotate(down_parts[0], "fs")
    down_parts[1] = [swap_fs(down_parts[1])]
    new_up, hidden = up_rows(me, rows, up_parts, gate)
    new_down = None
    partials = []
    for k, (low, _) in enumerate(cuts):
        new_down, partial = down_rows(me, hidden, rows, down_parts[k], low, width, new_down)
        partials.append(
            [partial[0]]
            + [
                lax.ppermute(term, "tp", list(enumerate(places)))
                for term, places in zip(partial[1:], source[1:])
            ]
        )
    backs = []
    for partial in partials:
        summed = add(fs, partial)
        backs.append(swap_fs(summed))
    mixed = pl.pallas_call(
        functools.partial(final_kernel, fs, tp),
        out_shape=jax.ShapeDtypeStruct((count, width), bf16),
        compiler_params=grant(16),
        cost_estimate=cost(2 * count * count * width, 4 * count * width),
    )(ids, *backs)
    return (mixed, new_gate[None], new_up[None], new_down[None])


def solution(mesh):
    in_specs = (
        P(("fs", "tp"), None),
        P("fs"),
        P(None, "fs", "tp"),
        P(None, "fs", "tp"),
        P(None, "fs", "tp"),
        P(("fs", "tp"), None),
        P(("fs", "tp"), None),
    )
    out_specs = (
        P(("fs", "tp"), None),
        P(("fs", "tp"), None, None),
        P(("fs", "tp"), None, None),
        P(("fs", "tp"), None, None),
    )

    return jax.shard_map(shards, mesh=mesh, in_specs=in_specs, out_specs=out_specs, check_vma=False)
```

```python
import functools

import jax
import jax.numpy as jnp
from jax import lax
from jax.experimental import pallas as pl
from jax.experimental.pallas import tpu as pltpu
from jax.sharding import PartitionSpec as P


norm_eps = 1e-06
lanes = 128
bf16 = jnp.bfloat16
f32 = jnp.float32


def cuts_of(width):
    first = width // 8 * 5
    return [(0, first), (first, width)]


def grant(mib):
    return pltpu.CompilerParams(vmem_limit_bytes=mib * 1024 * 1024)


def far_first(n):
    return sorted(range(1, n), key=lambda r: (abs(2 * r - n), r))


def cost(flops, nbytes):
    return pl.CostEstimate(flops=int(flops), bytes_accessed=int(nbytes), transcendentals=0)


def whole(shape):
    return pl.BlockSpec(shape, lambda *_: (0,) * len(shape))


def square(n):
    return lax.broadcasted_iota(jnp.int32, (n, n), 0), lax.broadcasted_iota(jnp.int32, (n, n), 1)


def to_col(row):
    n = row.shape[1]
    down, across = square(n)
    return jnp.sum(jnp.where(down == across, row, jnp.zeros((), row.dtype)), axis=1, keepdims=True)


def slot_onehot(group_row, fs):
    count = group_row.shape[1]
    down, across = square(count)
    group_col = to_col(group_row)
    earlier = jnp.where((group_col == group_row) & (across < down), 1.0, 0.0)
    rank = jnp.sum(earlier, axis=1, keepdims=True)
    slot = (group_col * float(count // fs) + rank).astype(jnp.int32)
    return jnp.where(slot == across, 1.0, 0.0).astype(bf16)


def group_of(ids, fs, tp):
    group = jnp.zeros(ids.shape, f32)
    for bound in range(1, fs):
        group = group + jnp.where(ids >= bound * tp, 1.0, 0.0)
    return group


def prep_kernel(fs, tp, tok_ref, ids_ref, weight_ref, out_ref):
    count, width = tok_ref.shape
    group = group_of(ids_ref[0:1, :], fs, tp)
    onehot = slot_onehot(group, fs)
    wide = tok_ref[...].astype(f32)
    scale = lax.rsqrt(jnp.mean(wide * wide, axis=-1, keepdims=True) + norm_eps)
    normed = (wide * scale).astype(bf16)
    lane = lax.broadcasted_iota(jnp.int32, (count, lanes), 1)
    extra = jnp.zeros((count, lanes), f32)
    for pick in range(2):
        local = ids_ref[pick : pick + 1, :].astype(f32) - group * float(tp)
        local = to_col(local).astype(jnp.int32)
        rest = to_col(weight_ref[pick : pick + 1, :])
        for part in range(3):
            piece = rest.astype(bf16).astype(f32)
            extra = extra + jnp.where(lane == local + part * tp, piece, 0.0)
            rest = rest - piece
    dims = (((0,), (0,)), ((), ()))
    rows = lax.dot_general(onehot, normed, dims, preferred_element_type=f32).astype(bf16)
    extra = lax.dot_general(onehot, extra.astype(bf16), dims, preferred_element_type=f32).astype(bf16)
    out_ref[:, :width] = rows
    out_ref[:, width:] = extra


def add_kernel(*refs):
    out_ref = refs[-1]
    fs, each, _ = out_ref.shape
    total = sum(ref[...].astype(f32) for ref in refs[:-1]).astype(bf16)
    for i in range(fs):
        out_ref[i] = total[i * each : (i + 1) * each]


def add(fs, terms):
    count, width = terms[0].shape
    return pl.pallas_call(
        add_kernel,
        out_shape=jax.ShapeDtypeStruct((fs, count // fs, width), bf16),
        compiler_params=grant(8),
        cost_estimate=cost(1e9, 2 * (len(terms) + 1) * count * width),
    )(*terms)


def cast_kernel(steps, scaled, squeeze, me_ref, in_ref, *refs):
    step = pl.program_id(0)
    value = in_ref[:, 0] if squeeze else in_ref[0]
    if scaled:
        value = value * to_col(refs[0][...])[None]
        refs = refs[1:]
    value = value.astype(bf16)
    for k in range(steps):

        @pl.when(step == k)
        def _(k=k):
            refs[k][...] = value


def cast_along(me, matrix, scale, axis, distances, params):
    fs, tp, rows, cols = matrix.shape
    steps = len(distances)

    def target(k, m):
        ahead = jnp.int32(distances[0])
        for j in range(1, steps):
            ahead = jnp.where(k == j, jnp.int32(distances[j]), ahead)
        return lax.rem(m[axis] + ahead, (fs, tp)[axis])

    if axis == 0:
        in_spec = pl.BlockSpec((1, tp, rows, cols), lambda k, m: (target(k, m), 0, 0, 0))
        shape = (tp, rows, cols)
    else:
        in_spec = pl.BlockSpec((fs, 1, rows, cols), lambda k, m: (0, target(k, m), 0, 0))
        shape = (fs, rows, cols)
    in_specs, args = [in_spec], [matrix]
    if scale is not None:
        in_specs.append(whole(scale.shape))
        args.append(scale)
    return pl.pallas_call(
        functools.partial(cast_kernel, steps, scale is not None, axis == 1),
        grid_spec=pltpu.PrefetchScalarGridSpec(
            num_scalar_prefetch=1, grid=(steps,), in_specs=in_specs, out_specs=[whole(shape)] * steps
        ),
        out_shape=[jax.ShapeDtypeStruct(shape, bf16)] * steps,
        compiler_params=params,
        cost_estimate=cost(1e9, 6 * matrix.size * steps // (fs, tp)[axis]),
    )(me, *args)


def in_order(me_ref, tp, action):
    for value in range(tp):

        @pl.when(me_ref[1] == value)
        def _(value=value):
            action([(value - j) % tp for j in range(tp)])


def merge_kernel(fs, tp, cuts, me_ref, *refs):
    ins, outs = refs[:tp], refs[tp:]

    def store(order):
        for r in range(fs):
            group = lax.rem(me_ref[0] + r, fs)
            full = jnp.concatenate([ins[q][group] for q in order], axis=-1)
            low, high = cuts[0]
            outs[r][...] = full[:, low:high]
            for out, (low, high) in zip(outs[fs:], cuts[1:]):
                out[group] = full[:, low:high]

    in_order(me_ref, tp, store)


def merge(me, parts, cuts):
    tp = len(parts)
    fs, rows, _ = parts[0].shape
    sizes = [high - low for low, high in cuts]
    shapes = [(rows, sizes[0])] * fs + [(fs, rows, size) for size in sizes[1:]]
    outs = pl.pallas_call(
        functools.partial(merge_kernel, fs, tp, cuts),
        grid_spec=pltpu.PrefetchScalarGridSpec(
            num_scalar_prefetch=1,
            grid=(1,),
            in_specs=[whole(parts[0].shape)] * tp,
            out_specs=[whole(shape) for shape in shapes],
        ),
        out_shape=[jax.ShapeDtypeStruct(shape, bf16) for shape in shapes],
        compiler_params=grant(16),
        cost_estimate=cost(1e9, 4 * tp * parts[0].size),
    )(me, *parts)
    return [outs[:fs], *outs[fs:]]


def regroup_kernel(fs, tp, me_ref, *refs):
    for q in range(tp):
        target = lax.rem(me_ref[1] + q, tp)
        for r in range(fs):
            refs[fs + q][r] = refs[r][target]


def regroup(me, parts):
    fs = len(parts)
    tp, rows, cols = parts[0].shape
    shape = (fs, rows, cols)
    return pl.pallas_call(
        functools.partial(regroup_kernel, fs, tp),
        grid_spec=pltpu.PrefetchScalarGridSpec(
            num_scalar_prefetch=1,
            grid=(1,),
            in_specs=[whole(parts[0].shape)] * fs,
            out_specs=[whole(shape)] * tp,
        ),
        out_shape=[jax.ShapeDtypeStruct(shape, bf16)] * tp,
        compiler_params=grant(16),
        cost_estimate=cost(1e9, 4 * fs * parts[0].size),
    )(me, *parts)


def product_of(x_refs, matrix_ref, rows_ref):
    width = matrix_ref.shape[0]
    count = x_refs[0].shape[0]
    for q, ref in enumerate(x_refs):
        rows_ref[q * count : (q + 1) * count, :] = ref[:, :width]
    return jnp.dot(rows_ref[...], matrix_ref[...], preferred_element_type=f32)


def gate_kernel(fs, tp, me_ref, *refs):
    x_refs, parts, (matrix_ref, out_ref, rows_ref) = refs[:tp], refs[tp : 2 * tp], refs[2 * tp :]
    height = parts[0].shape[1]

    def store(order):
        for r in range(fs):
            origin = lax.rem(me_ref[0] - r + fs, fs)
            matrix_ref[pl.ds(pl.multiple_of(origin * height, height), height), :] = jnp.concatenate(
                [parts[q][r] for q in order], axis=-1
            )

    in_order(me_ref, tp, store)
    out_ref[...] = product_of(x_refs, matrix_ref, rows_ref)


def gate_rows(me, rows, parts):
    tp = len(parts)
    fs, height, cols = parts[0].shape
    matrix = (fs * height, tp * cols)
    out = (tp * rows[0].shape[0], tp * cols)
    return pl.pallas_call(
        functools.partial(gate_kernel, fs, tp),
        grid_spec=pltpu.PrefetchScalarGridSpec(
            num_scalar_prefetch=1,
            grid=(1,),
            in_specs=[whole(rows[0].shape)] * tp + [whole(parts[0].shape)] * tp,
            out_specs=[whole(matrix), whole(out)],
            scratch_shapes=[pltpu.VMEM((out[0], matrix[0]), bf16)],
        ),
        out_shape=[jax.ShapeDtypeStruct(matrix, bf16), jax.ShapeDtypeStruct(out, f32)],
        compiler_params=grant(24),
        cost_estimate=cost(2 * out[0] * matrix[0] * matrix[1], 4 * matrix[0] * matrix[1]),
    )(me, *rows, *parts)


def assemble(me_ref, parts, matrix_ref):
    fs, rows = len(parts), parts[0].shape[0]
    if fs == 1:
        matrix_ref[...] = parts[0][...]
        return
    for r in range(fs):
        origin = lax.rem(me_ref[0] - r + fs, fs)
        matrix_ref[pl.ds(pl.multiple_of(origin * rows, rows), rows), :] = parts[r][...]


def up_kernel(tp, me_ref, *refs):
    x_refs, parts, refs = refs[:tp], refs[tp:-4], refs[-4:]
    gate_ref, matrix_ref, out_ref, rows_ref = refs
    assemble(me_ref, parts, matrix_ref)
    up = product_of(x_refs, matrix_ref, rows_ref)
    gate = gate_ref[...]
    out_ref[...] = (gate / (1.0 + jnp.exp(-gate)) * up).astype(bf16)


def up_rows(me, rows, parts, gate):
    tp = len(rows)
    matrix = (len(parts) * parts[0].shape[0], parts[0].shape[1])
    return pl.pallas_call(
        functools.partial(up_kernel, tp),
        grid_spec=pltpu.PrefetchScalarGridSpec(
            num_scalar_prefetch=1,
            grid=(1,),
            in_specs=[whole(rows[0].shape)] * tp
            + [whole(part.shape) for part in parts]
            + [whole(gate.shape)],
            out_specs=[whole(matrix), whole(gate.shape)],
            scratch_shapes=[pltpu.VMEM((gate.shape[0], matrix[0]), bf16)],
        ),
        out_shape=[jax.ShapeDtypeStruct(matrix, bf16), jax.ShapeDtypeStruct(gate.shape, bf16)],
        compiler_params=grant(24),
        cost_estimate=cost(2 * gate.size * matrix[0], 4 * matrix[0] * matrix[1]),
    )(me, *rows, *parts, gate)


def down_kernel(count_parts, tp, low, aliased, me_ref, hidden_ref, *refs):
    w_refs, refs = refs[:tp], refs[tp:]
    parts, refs = refs[:count_parts], refs[count_parts:]
    if aliased:
        refs = refs[1:]
    matrix_ref, outs, block, done = refs[0], refs[1 : 1 + tp], refs[1 + tp], refs[2 + tp]
    assemble(me_ref, parts, block)
    copy = pltpu.make_async_copy(block, matrix_ref.at[:, pl.ds(low, block.shape[1])], done)
    copy.start()
    product = jnp.dot(hidden_ref[...], block[...], preferred_element_type=f32)
    product = product.astype(bf16).astype(f32)
    count = w_refs[0].shape[0]
    lane = lax.broadcasted_iota(jnp.int32, (count, lanes), 1)
    mine = me_ref[1]
    chosen = (lane == mine) | (lane == mine + tp) | (lane == mine + 2 * tp)
    for q in range(tp):
        weight = jnp.sum(
            jnp.where(chosen, w_refs[q][...].astype(f32), 0.0), axis=1, keepdims=True
        )
        outs[q][...] = (product[q * count : (q + 1) * count] * weight).astype(bf16)
    copy.wait()


def down_rows(me, hidden, rows, parts, low, width, prior):
    tp = len(rows)
    count = rows[0].shape[0]
    depth = hidden.shape[1]
    size = parts[0].shape[1]
    weight_block = width // lanes
    in_specs = [whole(hidden.shape)]
    in_specs += [pl.BlockSpec((count, lanes), lambda k, m: (0, weight_block))] * tp
    in_specs += [whole(part.shape) for part in parts]
    args = [hidden, *rows, *parts]
    aliases = {}
    if prior is not None:
        in_specs.append(pl.BlockSpec(memory_space=pl.ANY))
        args.append(prior)
        aliases = {len(args): 0}
    outs = pl.pallas_call(
        functools.partial(down_kernel, len(parts), tp, low, prior is not None),
        grid_spec=pltpu.PrefetchScalarGridSpec(
            num_scalar_prefetch=1,
            grid=(1,),
            in_specs=in_specs,
            out_specs=[pl.BlockSpec(memory_space=pl.ANY)] + [whole((count, size))] * tp,
            scratch_shapes=[pltpu.VMEM((depth, size), bf16), pltpu.SemaphoreType.DMA],
        ),
        out_shape=[jax.ShapeDtypeStruct((depth, width), bf16)]
        + [jax.ShapeDtypeStruct((count, size), bf16)] * tp,
        input_output_aliases=aliases,
        compiler_params=grant(16),
        cost_estimate=cost(2 * tp * count * depth * size, 4 * depth * size),
    )(me, *args)
    return outs[0], outs[1:]


def final_kernel(fs, tp, ids_ref, *refs):
    ins, out_ref = refs[:-1], refs[-1]
    onehot = slot_onehot(group_of(ids_ref[0:1, :], fs, tp), fs)
    low = 0
    for ref in ins:
        high = low + ref.shape[1]
        out_ref[:, low:high] = jnp.dot(onehot, ref[...], preferred_element_type=f32).astype(bf16)
        low = high


def shards(tokens, norm_gain, gate_proj, up_proj, down_proj, expert_ids, route_weight):
    fs = lax.axis_size("fs")
    tp = lax.axis_size("tp")
    me = jnp.stack([lax.axis_index("fs"), lax.axis_index("tp")]).astype(jnp.int32)
    count, width = tokens.shape
    cuts = cuts_of(width)

    def rotate(parts, axis, distances=None):
        n = len(parts)
        out = list(parts)
        for r in distances or far_first(n):
            out[r] = lax.ppermute(parts[r], axis, [(k, (k + r) % n) for k in range(n)])
        return out

    def swap_fs(value):
        out = lax.all_to_all(value, "fs", 0, 0, tiled=True)
        return out.reshape(-1, out.shape[2])

    def by_expert(matrix):
        return matrix.reshape((fs, tp) + matrix.shape[1:])

    ids, weights = expert_ids.T, route_weight.T
    scale = norm_gain[None, :]

    sent = pl.pallas_call(
        functools.partial(prep_kernel, fs, tp),
        out_shape=jax.ShapeDtypeStruct((count, width + lanes), bf16),
        cost_estimate=cost(2 * count * count * width, 4 * count * width),
    )(tokens, ids, weights)
    landed = swap_fs(sent.reshape(fs, count // fs, -1))
    gate_parts = [None] * fs
    early, late = far_first(fs)[:3], far_first(fs)[3:]

    def cut_gate(distances, params):
        cut = cast_along(me, by_expert(gate_proj), scale, 0, distances, params)
        for r, part in zip(distances, cut):
            gate_parts[r] = part
        gate_parts[:] = rotate(gate_parts, "fs", distances=[r for r in distances if r > 0])

    cut_gate(early, None)
    up_parts = cast_along(me, by_expert(up_proj), scale, 1, range(tp), grant(16))
    up_parts = rotate(up_parts, "tp")
    cut_gate(late + [0], grant(16))
    down_parts = cast_along(me, by_expert(down_proj), None, 1, range(tp), grant(16))
    down_parts = rotate(down_parts, "tp")
    source = [
        [((j ^ core) - step) % tp for j in range(tp)] for core in (0, 1) for step in range(0, tp, 2)
    ]
    rows = [landed] + [
        lax.ppermute(landed, "tp", [(k, (k + step) % tp) for k in range(tp)])
        for step in range(2, tp, 2)
    ]
    rows += [lax.ppermute(part, "tp", [(k, k ^ 1) for k in range(tp)]) for part in rows]
    (up_parts,) = merge(me, up_parts, [(0, tp * up_parts[0].shape[2])])
    up_parts = rotate(up_parts, "fs")
    gate_parts = regroup(me, gate_parts)
    gate_parts = rotate(gate_parts, "tp")
    down_parts = merge(me, down_parts, cuts)
    new_gate, gate = gate_rows(me, rows, gate_parts)
    down_parts[0] = rotate(down_parts[0], "fs")
    down_parts[1] = [swap_fs(down_parts[1])]
    new_up, hidden = up_rows(me, rows, up_parts, gate)
    new_down = None
    partials = []
    for k, (low, _) in enumerate(cuts):
        new_down, partial = down_rows(me, hidden, rows, down_parts[k], low, width, new_down)
        partials.append(
            [partial[0]]
            + [
                lax.ppermute(term, "tp", list(enumerate(places)))
                for term, places in zip(partial[1:], source[1:])
            ]
        )
    backs = []
    for partial in partials:
        summed = add(fs, partial)
        backs.append(swap_fs(summed))
    mixed = pl.pallas_call(
        functools.partial(final_kernel, fs, tp),
        out_shape=jax.ShapeDtypeStruct((count, width), bf16),
        compiler_params=grant(16),
        cost_estimate=cost(2 * count * count * width, 4 * count * width),
    )(ids, *backs)
    return (mixed, new_gate[None], new_up[None], new_down[None])


def solution(mesh):
    in_specs = (
        P(("fs", "tp"), None),
        P("fs"),
        P(None, "fs", "tp"),
        P(None, "fs", "tp"),
        P(None, "fs", "tp"),
        P(("fs", "tp"), None),
        P(("fs", "tp"), None),
    )
    out_specs = (
        P(("fs", "tp"), None),
        P(("fs", "tp"), None, None),
        P(("fs", "tp"), None, None),
        P(("fs", "tp"), None, None),
    )

    return jax.shard_map(shards, mesh=mesh, in_specs=in_specs, out_specs=out_specs, check_vma=False)
```

```python
import functools

import jax
import jax.numpy as jnp
from jax import lax
from jax.experimental import pallas as pl
from jax.experimental.pallas import tpu as pltpu
from jax.sharding import PartitionSpec as P


norm_eps = 1e-06
lanes = 128
bf16 = jnp.bfloat16
f32 = jnp.float32


def cuts_of(width):
    first = width // 2
    return [(0, first), (first, width)]


def grant(mib):
    return pltpu.CompilerParams(vmem_limit_bytes=mib * 1024 * 1024)


def far_first(n):
    return sorted(range(1, n), key=lambda r: (abs(2 * r - n), r))


def cost(flops, nbytes):
    return pl.CostEstimate(flops=int(flops), bytes_accessed=int(nbytes), transcendentals=0)


def whole(shape):
    return pl.BlockSpec(shape, lambda *_: (0,) * len(shape))


def square(n):
    return lax.broadcasted_iota(jnp.int32, (n, n), 0), lax.broadcasted_iota(jnp.int32, (n, n), 1)


def to_col(row):
    n = row.shape[1]
    down, across = square(n)
    return jnp.sum(jnp.where(down == across, row, jnp.zeros((), row.dtype)), axis=1, keepdims=True)


def slot_onehot(group_row, fs):
    count = group_row.shape[1]
    down, across = square(count)
    group_col = to_col(group_row)
    earlier = jnp.where((group_col == group_row) & (across < down), 1.0, 0.0)
    rank = jnp.sum(earlier, axis=1, keepdims=True)
    slot = (group_col * float(count // fs) + rank).astype(jnp.int32)
    return jnp.where(slot == across, 1.0, 0.0).astype(bf16)


def group_of(ids, fs, tp):
    group = jnp.zeros(ids.shape, f32)
    for bound in range(1, fs):
        group = group + jnp.where(ids >= bound * tp, 1.0, 0.0)
    return group


def prep_kernel(fs, tp, tok_ref, ids_ref, weight_ref, out_ref):
    count, width = tok_ref.shape
    group = group_of(ids_ref[0:1, :], fs, tp)
    onehot = slot_onehot(group, fs)
    wide = tok_ref[...].astype(f32)
    scale = lax.rsqrt(jnp.mean(wide * wide, axis=-1, keepdims=True) + norm_eps)
    normed = (wide * scale).astype(bf16)
    lane = lax.broadcasted_iota(jnp.int32, (count, lanes), 1)
    extra = jnp.zeros((count, lanes), f32)
    for pick in range(2):
        local = ids_ref[pick : pick + 1, :].astype(f32) - group * float(tp)
        local = to_col(local).astype(jnp.int32)
        rest = to_col(weight_ref[pick : pick + 1, :])
        for part in range(3):
            piece = rest.astype(bf16).astype(f32)
            extra = extra + jnp.where(lane == local + part * tp, piece, 0.0)
            rest = rest - piece
    dims = (((0,), (0,)), ((), ()))
    rows = lax.dot_general(onehot, normed, dims, preferred_element_type=f32).astype(bf16)
    extra = lax.dot_general(onehot, extra.astype(bf16), dims, preferred_element_type=f32).astype(bf16)
    out_ref[:, :width] = rows
    out_ref[:, width:] = extra


def fold_kernel(mine_ref, other_ref, *outs):
    count = outs[0].shape[0]
    for k, out in enumerate(outs):
        block = slice(k * count, (k + 1) * count)
        out[...] = (mine_ref[block].astype(f32) + other_ref[block].astype(f32)).astype(bf16)


def fold(count, mine, other):
    rows, width = mine.shape
    return pl.pallas_call(
        fold_kernel,
        out_shape=[jax.ShapeDtypeStruct((count, width), bf16)] * (rows // count),
        compiler_params=grant(8),
        cost_estimate=cost(1e9, 6 * rows * width),
    )(mine, other)


def add_kernel(*refs):
    out_ref = refs[-1]
    fs, each, _ = out_ref.shape
    total = sum(ref[...].astype(f32) for ref in refs[:-1]).astype(bf16)
    for i in range(fs):
        out_ref[i] = total[i * each : (i + 1) * each]


def add(fs, terms):
    count, width = terms[0].shape
    return pl.pallas_call(
        add_kernel,
        out_shape=jax.ShapeDtypeStruct((fs, count // fs, width), bf16),
        compiler_params=grant(8),
        cost_estimate=cost(1e9, 2 * (len(terms) + 1) * count * width),
    )(*terms)


def cast_kernel(steps, scaled, squeeze, me_ref, in_ref, *refs):
    step = pl.program_id(0)
    value = in_ref[:, 0] if squeeze else in_ref[0]
    if scaled:
        value = value * to_col(refs[0][...])[None]
        refs = refs[1:]
    value = value.astype(bf16)
    for k in range(steps):

        @pl.when(step == k)
        def _(k=k):
            refs[k][...] = value


def cast_along(me, matrix, scale, axis, distances, params):
    fs, tp, rows, cols = matrix.shape
    steps = len(distances)

    def target(k, m):
        ahead = jnp.int32(distances[0])
        for j in range(1, steps):
            ahead = jnp.where(k == j, jnp.int32(distances[j]), ahead)
        return lax.rem(m[axis] + ahead, (fs, tp)[axis])

    if axis == 0:
        in_spec = pl.BlockSpec((1, tp, rows, cols), lambda k, m: (target(k, m), 0, 0, 0))
        shape = (tp, rows, cols)
    else:
        in_spec = pl.BlockSpec((fs, 1, rows, cols), lambda k, m: (0, target(k, m), 0, 0))
        shape = (fs, rows, cols)
    in_specs, args = [in_spec], [matrix]
    if scale is not None:
        in_specs.append(whole(scale.shape))
        args.append(scale)
    return pl.pallas_call(
        functools.partial(cast_kernel, steps, scale is not None, axis == 1),
        grid_spec=pltpu.PrefetchScalarGridSpec(
            num_scalar_prefetch=1, grid=(steps,), in_specs=in_specs, out_specs=[whole(shape)] * steps
        ),
        out_shape=[jax.ShapeDtypeStruct(shape, bf16)] * steps,
        compiler_params=params,
        cost_estimate=cost(1e9, 6 * matrix.size * steps // (fs, tp)[axis]),
    )(me, *args)


def in_order(me_ref, tp, action):
    for value in range(tp):

        @pl.when(me_ref[1] == value)
        def _(value=value):
            action([(value - j) % tp for j in range(tp)])


def merge_kernel(fs, tp, cuts, me_ref, *refs):
    ins, outs = refs[:tp], refs[tp:]

    def store(order):
        for r in range(fs):
            group = lax.rem(me_ref[0] + r, fs)
            full = jnp.concatenate([ins[q][group] for q in order], axis=-1)
            for k, (low, high) in enumerate(cuts):
                outs[k * fs + r][...] = full[:, low:high]

    in_order(me_ref, tp, store)


def merge(me, parts, cuts):
    tp = len(parts)
    fs, rows, _ = parts[0].shape
    shapes = [(rows, high - low) for low, high in cuts for _ in range(fs)]
    outs = pl.pallas_call(
        functools.partial(merge_kernel, fs, tp, cuts),
        grid_spec=pltpu.PrefetchScalarGridSpec(
            num_scalar_prefetch=1,
            grid=(1,),
            in_specs=[whole(parts[0].shape)] * tp,
            out_specs=[whole(shape) for shape in shapes],
        ),
        out_shape=[jax.ShapeDtypeStruct(shape, bf16) for shape in shapes],
        compiler_params=grant(16),
        cost_estimate=cost(1e9, 4 * tp * parts[0].size),
    )(me, *parts)
    return [outs[k * fs : (k + 1) * fs] for k in range(len(cuts))]


def regroup_kernel(fs, tp, me_ref, *refs):
    for q in range(tp):
        target = lax.rem(me_ref[1] + q, tp)
        for r in range(fs):
            refs[fs + q][r] = refs[r][target]


def regroup(me, parts):
    fs = len(parts)
    tp, rows, cols = parts[0].shape
    shape = (fs, rows, cols)
    return pl.pallas_call(
        functools.partial(regroup_kernel, fs, tp),
        grid_spec=pltpu.PrefetchScalarGridSpec(
            num_scalar_prefetch=1,
            grid=(1,),
            in_specs=[whole(parts[0].shape)] * fs,
            out_specs=[whole(shape)] * tp,
        ),
        out_shape=[jax.ShapeDtypeStruct(shape, bf16)] * tp,
        compiler_params=grant(16),
        cost_estimate=cost(1e9, 4 * fs * parts[0].size),
    )(me, *parts)


def product_of(x_refs, matrix_ref, rows_ref):
    width = matrix_ref.shape[0]
    count = x_refs[0].shape[0]
    for q, ref in enumerate(x_refs):
        rows_ref[q * count : (q + 1) * count, :] = ref[:, :width]
    return jnp.dot(rows_ref[...], matrix_ref[...], preferred_element_type=f32)


def gate_kernel(fs, tp, me_ref, *refs):
    x_refs, parts, (matrix_ref, out_ref, rows_ref) = refs[:tp], refs[tp : 2 * tp], refs[2 * tp :]
    height = parts[0].shape[1]

    def store(order):
        for r in range(fs):
            origin = lax.rem(me_ref[0] - r + fs, fs)
            matrix_ref[pl.ds(pl.multiple_of(origin * height, height), height), :] = jnp.concatenate(
                [parts[q][r] for q in order], axis=-1
            )

    in_order(me_ref, tp, store)
    out_ref[...] = product_of(x_refs, matrix_ref, rows_ref)


def gate_rows(me, rows, parts):
    tp = len(parts)
    fs, height, cols = parts[0].shape
    matrix = (fs * height, tp * cols)
    out = (tp * rows[0].shape[0], tp * cols)
    return pl.pallas_call(
        functools.partial(gate_kernel, fs, tp),
        grid_spec=pltpu.PrefetchScalarGridSpec(
            num_scalar_prefetch=1,
            grid=(1,),
            in_specs=[whole(rows[0].shape)] * tp + [whole(parts[0].shape)] * tp,
            out_specs=[whole(matrix), whole(out)],
            scratch_shapes=[pltpu.VMEM((out[0], matrix[0]), bf16)],
        ),
        out_shape=[jax.ShapeDtypeStruct(matrix, bf16), jax.ShapeDtypeStruct(out, f32)],
        compiler_params=grant(24),
        cost_estimate=cost(2 * out[0] * matrix[0] * matrix[1], 4 * matrix[0] * matrix[1]),
    )(me, *rows, *parts)


def assemble(me_ref, parts, matrix_ref):
    fs, rows = len(parts), parts[0].shape[0]
    if fs == 1:
        matrix_ref[...] = parts[0][...]
        return
    for r in range(fs):
        origin = lax.rem(me_ref[0] - r + fs, fs)
        matrix_ref[pl.ds(pl.multiple_of(origin * rows, rows), rows), :] = parts[r][...]


def up_kernel(tp, me_ref, *refs):
    x_refs, parts, refs = refs[:tp], refs[tp:-4], refs[-4:]
    gate_ref, matrix_ref, out_ref, rows_ref = refs
    assemble(me_ref, parts, matrix_ref)
    up = product_of(x_refs, matrix_ref, rows_ref)
    gate = gate_ref[...]
    out_ref[...] = (gate / (1.0 + jnp.exp(-gate)) * up).astype(bf16)


def up_rows(me, rows, parts, gate):
    tp = len(rows)
    matrix = (len(parts) * parts[0].shape[0], parts[0].shape[1])
    return pl.pallas_call(
        functools.partial(up_kernel, tp),
        grid_spec=pltpu.PrefetchScalarGridSpec(
            num_scalar_prefetch=1,
            grid=(1,),
            in_specs=[whole(rows[0].shape)] * tp
            + [whole(part.shape) for part in parts]
            + [whole(gate.shape)],
            out_specs=[whole(matrix), whole(gate.shape)],
            scratch_shapes=[pltpu.VMEM((gate.shape[0], matrix[0]), bf16)],
        ),
        out_shape=[jax.ShapeDtypeStruct(matrix, bf16), jax.ShapeDtypeStruct(gate.shape, bf16)],
        compiler_params=grant(24),
        cost_estimate=cost(2 * gate.size * matrix[0], 4 * matrix[0] * matrix[1]),
    )(me, *rows, *parts, gate)


def down_kernel(count_parts, tp, low, aliased, me_ref, hidden_ref, *refs):
    w_refs, refs = refs[:tp], refs[tp:]
    parts, refs = refs[:count_parts], refs[count_parts:]
    if aliased:
        refs = refs[1:]
    matrix_ref, same_ref, other_ref, block, done = refs
    assemble(me_ref, parts, block)
    copy = pltpu.make_async_copy(block, matrix_ref.at[:, pl.ds(low, block.shape[1])], done)
    copy.start()
    product = jnp.dot(hidden_ref[...], block[...], preferred_element_type=f32)
    product = product.astype(bf16).astype(f32)
    count = w_refs[0].shape[0]
    lane = lax.broadcasted_iota(jnp.int32, (count, lanes), 1)
    mine = me_ref[1]
    chosen = (lane == mine) | (lane == mine + tp) | (lane == mine + 2 * tp)
    for q in range(tp):
        weight = jnp.sum(
            jnp.where(chosen, w_refs[q][...].astype(f32), 0.0), axis=1, keepdims=True
        )
        out_ref, at = (same_ref, q) if q < tp // 2 else (other_ref, q - tp // 2)
        out_ref[at * count : (at + 1) * count] = (
            product[q * count : (q + 1) * count] * weight
        ).astype(bf16)
    copy.wait()


def down_rows(me, hidden, rows, parts, low, width, prior):
    tp = len(rows)
    count = rows[0].shape[0]
    depth = hidden.shape[1]
    size = parts[0].shape[1]
    weight_block = width // lanes
    in_specs = [whole(hidden.shape)]
    in_specs += [pl.BlockSpec((count, lanes), lambda k, m: (0, weight_block))] * tp
    in_specs += [whole(part.shape) for part in parts]
    args = [hidden, *rows, *parts]
    aliases = {}
    if prior is not None:
        in_specs.append(pl.BlockSpec(memory_space=pl.ANY))
        args.append(prior)
        aliases = {len(args): 0}
    outs = pl.pallas_call(
        functools.partial(down_kernel, len(parts), tp, low, prior is not None),
        grid_spec=pltpu.PrefetchScalarGridSpec(
            num_scalar_prefetch=1,
            grid=(1,),
            in_specs=in_specs,
            out_specs=[pl.BlockSpec(memory_space=pl.ANY)] + [whole((tp // 2 * count, size))] * 2,
            scratch_shapes=[pltpu.VMEM((depth, size), bf16), pltpu.SemaphoreType.DMA],
        ),
        out_shape=[jax.ShapeDtypeStruct((depth, width), bf16)]
        + [jax.ShapeDtypeStruct((tp // 2 * count, size), bf16)] * 2,
        input_output_aliases=aliases,
        compiler_params=grant(16),
        cost_estimate=cost(2 * tp * count * depth * size, 4 * depth * size),
    )(me, *args)
    return outs


def final_kernel(fs, tp, ids_ref, *refs):
    ins, out_ref = refs[:-1], refs[-1]
    onehot = slot_onehot(group_of(ids_ref[0:1, :], fs, tp), fs)
    low = 0
    for ref in ins:
        high = low + ref.shape[1]
        out_ref[:, low:high] = jnp.dot(onehot, ref[...], preferred_element_type=f32).astype(bf16)
        low = high


def shards(tokens, norm_gain, gate_proj, up_proj, down_proj, expert_ids, route_weight):
    fs = lax.axis_size("fs")
    tp = lax.axis_size("tp")
    me = jnp.stack([lax.axis_index("fs"), lax.axis_index("tp")]).astype(jnp.int32)
    count, width = tokens.shape
    cuts = cuts_of(width)

    def rotate(parts, axis, distances=None):
        n = len(parts)
        out = list(parts)
        for r in distances or far_first(n):
            out[r] = lax.ppermute(parts[r], axis, [(k, (k + r) % n) for k in range(n)])
        return out

    def swap_fs(value):
        out = lax.all_to_all(value, "fs", 0, 0, tiled=True)
        return out.reshape(-1, out.shape[2])

    def swap_core(value):
        return lax.ppermute(value, "tp", [(j, j ^ 1) for j in range(tp)])

    def by_expert(matrix):
        return matrix.reshape((fs, tp) + matrix.shape[1:])

    ids, weights = expert_ids.T, route_weight.T
    scale = norm_gain[None, :]

    sent = pl.pallas_call(
        functools.partial(prep_kernel, fs, tp),
        out_shape=jax.ShapeDtypeStruct((count, width + lanes), bf16),
        cost_estimate=cost(2 * count * count * width, 4 * count * width),
    )(tokens, ids, weights)
    landed = swap_fs(sent.reshape(fs, count // fs, -1))
    gate_parts = [None] * fs
    early, late = far_first(fs)[:3], far_first(fs)[3:]

    def cut_gate(distances, params):
        cut = cast_along(me, by_expert(gate_proj), scale, 0, distances, params)
        for r, part in zip(distances, cut):
            gate_parts[r] = part
        gate_parts[:] = rotate(gate_parts, "fs", distances=[r for r in distances if r > 0])

    cut_gate(early, None)
    up_parts = cast_along(me, by_expert(up_proj), scale, 1, range(tp), grant(16))
    up_parts = rotate(up_parts, "tp")
    cut_gate(late + [0], grant(16))
    down_parts = cast_along(me, by_expert(down_proj), None, 1, range(tp), grant(16))
    down_parts = rotate(down_parts, "tp")
    rows = [landed] + [
        lax.ppermute(landed, "tp", [(k, (k + step) % tp) for k in range(tp)])
        for step in range(2, tp, 2)
    ]
    rows += [swap_core(part) for part in rows]
    (up_parts,) = merge(me, up_parts, [(0, tp * up_parts[0].shape[2])])
    up_parts = rotate(up_parts, "fs")
    gate_parts = regroup(me, gate_parts)
    gate_parts = rotate(gate_parts, "tp")
    down_parts = merge(me, down_parts, cuts)
    new_gate, gate = gate_rows(me, rows, gate_parts)
    down_parts[0] = rotate(down_parts[0], "fs")
    down_parts[1] = rotate(down_parts[1], "fs")
    new_up, hidden = up_rows(me, rows, up_parts, gate)
    new_down = None
    backs = []
    for k, (low, _) in enumerate(cuts):
        new_down, mine, other = down_rows(
            me, hidden, rows, down_parts[k], low, width, new_down
        )
        other = swap_core(other)
        terms = fold(count, mine, other)
        terms = [terms[0]] + [
            lax.ppermute(term, "tp", [(j, (j - step) % tp) for j in range(tp)])
            for term, step in zip(terms[1:], range(2, tp, 2))
        ]
        summed = add(fs, terms)
        backs.append(swap_fs(summed))
    mixed = pl.pallas_call(
        functools.partial(final_kernel, fs, tp),
        out_shape=jax.ShapeDtypeStruct((count, width), bf16),
        compiler_params=grant(16),
        cost_estimate=cost(2 * count * count * width, 4 * count * width),
    )(ids, *backs)
    return (mixed, new_gate[None], new_up[None], new_down[None])


def solution(mesh):
    in_specs = (
        P(("fs", "tp"), None),
        P("fs"),
        P(None, "fs", "tp"),
        P(None, "fs", "tp"),
        P(None, "fs", "tp"),
        P(("fs", "tp"), None),
        P(("fs", "tp"), None),
    )
    out_specs = (
        P(("fs", "tp"), None),
        P(("fs", "tp"), None, None),
        P(("fs", "tp"), None, None),
        P(("fs", "tp"), None, None),
    )

    return jax.shard_map(shards, mesh=mesh, in_specs=in_specs, out_specs=out_specs, check_vma=False)
```

```python
import functools

import jax
import jax.numpy as jnp
from jax import lax
from jax.experimental import pallas as pl
from jax.experimental.pallas import tpu as pltpu
from jax.sharding import PartitionSpec as P


norm_eps = 1e-06
lanes = 128
bf16 = jnp.bfloat16
f32 = jnp.float32


def cuts_of(width):
    first = width // 8 * 5
    return [(0, first), (first, width)]


def grant(mib):
    return pltpu.CompilerParams(vmem_limit_bytes=mib * 1024 * 1024)


def far_first(n):
    return sorted(range(1, n), key=lambda r: (abs(2 * r - n), r))


def cost(flops, nbytes):
    return pl.CostEstimate(flops=int(flops), bytes_accessed=int(nbytes), transcendentals=0)


def whole(shape):
    return pl.BlockSpec(shape, lambda *_: (0,) * len(shape))


def square(n):
    return lax.broadcasted_iota(jnp.int32, (n, n), 0), lax.broadcasted_iota(jnp.int32, (n, n), 1)


def to_col(row):
    n = row.shape[1]
    down, across = square(n)
    return jnp.sum(jnp.where(down == across, row, jnp.zeros((), row.dtype)), axis=1, keepdims=True)


def slot_onehot(group_row, fs):
    count = group_row.shape[1]
    down, across = square(count)
    group_col = to_col(group_row)
    earlier = jnp.where((group_col == group_row) & (across < down), 1.0, 0.0)
    rank = jnp.sum(earlier, axis=1, keepdims=True)
    slot = (group_col * float(count // fs) + rank).astype(jnp.int32)
    return jnp.where(slot == across, 1.0, 0.0).astype(bf16)


def group_of(ids, fs, tp):
    group = jnp.zeros(ids.shape, f32)
    for bound in range(1, fs):
        group = group + jnp.where(ids >= bound * tp, 1.0, 0.0)
    return group


def prep_kernel(fs, tp, tok_ref, ids_ref, weight_ref, out_ref):
    count, width = tok_ref.shape
    group = group_of(ids_ref[0:1, :], fs, tp)
    onehot = slot_onehot(group, fs)
    wide = tok_ref[...].astype(f32)
    scale = lax.rsqrt(jnp.mean(wide * wide, axis=-1, keepdims=True) + norm_eps)
    normed = (wide * scale).astype(bf16)
    lane = lax.broadcasted_iota(jnp.int32, (count, lanes), 1)
    extra = jnp.zeros((count, lanes), f32)
    for pick in range(2):
        local = ids_ref[pick : pick + 1, :].astype(f32) - group * float(tp)
        local = to_col(local).astype(jnp.int32)
        rest = to_col(weight_ref[pick : pick + 1, :])
        for part in range(3):
            piece = rest.astype(bf16).astype(f32)
            extra = extra + jnp.where(lane == local + part * tp, piece, 0.0)
            rest = rest - piece
    dims = (((0,), (0,)), ((), ()))
    rows = lax.dot_general(onehot, normed, dims, preferred_element_type=f32).astype(bf16)
    extra = lax.dot_general(onehot, extra.astype(bf16), dims, preferred_element_type=f32).astype(bf16)
    out_ref[:, :width] = rows
    out_ref[:, width:] = extra


def fold_kernel(mine_ref, other_ref, *outs):
    count = outs[0].shape[0]
    for k, out in enumerate(outs):
        block = slice(k * count, (k + 1) * count)
        out[...] = (mine_ref[block].astype(f32) + other_ref[block].astype(f32)).astype(bf16)


def fold(count, mine, other):
    rows, width = mine.shape
    return pl.pallas_call(
        fold_kernel,
        out_shape=[jax.ShapeDtypeStruct((count, width), bf16)] * (rows // count),
        compiler_params=grant(8),
        cost_estimate=cost(1e9, 6 * rows * width),
    )(mine, other)


def add_kernel(counts, *refs):
    refs, out_ref = list(refs[:-1]), refs[-1]
    fs, each, _ = out_ref.shape
    low = 0
    for count in counts:
        terms, refs = refs[:count], refs[count:]
        total = sum(ref[...].astype(f32) for ref in terms).astype(bf16)
        high = low + total.shape[1]
        for i in range(fs):
            out_ref[i, :, low:high] = total[i * each : (i + 1) * each]
        low = high


def add(fs, groups):
    count = groups[0][0].shape[0]
    width = sum(terms[0].shape[1] for terms in groups)
    flat = [term for terms in groups for term in terms]
    return pl.pallas_call(
        functools.partial(add_kernel, [len(terms) for terms in groups]),
        out_shape=jax.ShapeDtypeStruct((fs, count // fs, width), bf16),
        compiler_params=grant(8),
        cost_estimate=cost(1e9, 2 * (len(groups[0]) + 1) * count * width),
    )(*flat)


def cast_kernel(steps, scaled, squeeze, me_ref, in_ref, *refs):
    step = pl.program_id(0)
    value = in_ref[:, 0] if squeeze else in_ref[0]
    if scaled:
        value = value * to_col(refs[0][...])[None]
        refs = refs[1:]
    value = value.astype(bf16)
    for k in range(steps):

        @pl.when(step == k)
        def _(k=k):
            refs[k][...] = value


def cast_along(me, matrix, scale, axis, distances, params):
    fs, tp, rows, cols = matrix.shape
    steps = len(distances)

    def target(k, m):
        ahead = jnp.int32(distances[0])
        for j in range(1, steps):
            ahead = jnp.where(k == j, jnp.int32(distances[j]), ahead)
        return lax.rem(m[axis] + ahead, (fs, tp)[axis])

    if axis == 0:
        in_spec = pl.BlockSpec((1, tp, rows, cols), lambda k, m: (target(k, m), 0, 0, 0))
        shape = (tp, rows, cols)
    else:
        in_spec = pl.BlockSpec((fs, 1, rows, cols), lambda k, m: (0, target(k, m), 0, 0))
        shape = (fs, rows, cols)
    in_specs, args = [in_spec], [matrix]
    if scale is not None:
        in_specs.append(whole(scale.shape))
        args.append(scale)
    return pl.pallas_call(
        functools.partial(cast_kernel, steps, scale is not None, axis == 1),
        grid_spec=pltpu.PrefetchScalarGridSpec(
            num_scalar_prefetch=1, grid=(steps,), in_specs=in_specs, out_specs=[whole(shape)] * steps
        ),
        out_shape=[jax.ShapeDtypeStruct(shape, bf16)] * steps,
        compiler_params=params,
        cost_estimate=cost(1e9, 6 * matrix.size * steps // (fs, tp)[axis]),
    )(me, *args)


def in_order(me_ref, tp, action):
    for value in range(tp):

        @pl.when(me_ref[1] == value)
        def _(value=value):
            action([(value - j) % tp for j in range(tp)])


def merge_kernel(fs, tp, cuts, me_ref, *refs):
    ins, outs = refs[:tp], refs[tp:]

    def store(order):
        for r in range(fs):
            group = lax.rem(me_ref[0] + r, fs)
            full = jnp.concatenate([ins[q][group] for q in order], axis=-1)
            for k, (low, high) in enumerate(cuts):
                outs[k * fs + r][...] = full[:, low:high]

    in_order(me_ref, tp, store)


def merge(me, parts, cuts):
    tp = len(parts)
    fs, rows, _ = parts[0].shape
    shapes = [(rows, high - low) for low, high in cuts for _ in range(fs)]
    outs = pl.pallas_call(
        functools.partial(merge_kernel, fs, tp, cuts),
        grid_spec=pltpu.PrefetchScalarGridSpec(
            num_scalar_prefetch=1,
            grid=(1,),
            in_specs=[whole(parts[0].shape)] * tp,
            out_specs=[whole(shape) for shape in shapes],
        ),
        out_shape=[jax.ShapeDtypeStruct(shape, bf16) for shape in shapes],
        compiler_params=grant(16),
        cost_estimate=cost(1e9, 4 * tp * parts[0].size),
    )(me, *parts)
    return [outs[k * fs : (k + 1) * fs] for k in range(len(cuts))]


def regroup_kernel(fs, tp, me_ref, *refs):
    for q in range(tp):
        target = lax.rem(me_ref[1] + q, tp)
        for r in range(fs):
            refs[fs + q][r] = refs[r][target]


def regroup(me, parts):
    fs = len(parts)
    tp, rows, cols = parts[0].shape
    shape = (fs, rows, cols)
    return pl.pallas_call(
        functools.partial(regroup_kernel, fs, tp),
        grid_spec=pltpu.PrefetchScalarGridSpec(
            num_scalar_prefetch=1,
            grid=(1,),
            in_specs=[whole(parts[0].shape)] * fs,
            out_specs=[whole(shape)] * tp,
        ),
        out_shape=[jax.ShapeDtypeStruct(shape, bf16)] * tp,
        compiler_params=grant(16),
        cost_estimate=cost(1e9, 4 * fs * parts[0].size),
    )(me, *parts)


def product_of(x_refs, matrix_ref, rows_ref):
    width = matrix_ref.shape[0]
    count = x_refs[0].shape[0]
    for q, ref in enumerate(x_refs):
        rows_ref[q * count : (q + 1) * count, :] = ref[:, :width]
    return jnp.dot(rows_ref[...], matrix_ref[...], preferred_element_type=f32)


def gate_kernel(fs, tp, me_ref, *refs):
    x_refs, parts, (matrix_ref, out_ref, rows_ref) = refs[:tp], refs[tp : 2 * tp], refs[2 * tp :]
    height = parts[0].shape[1]

    def store(order):
        for r in range(fs):
            origin = lax.rem(me_ref[0] - r + fs, fs)
            matrix_ref[pl.ds(pl.multiple_of(origin * height, height), height), :] = jnp.concatenate(
                [parts[q][r] for q in order], axis=-1
            )

    in_order(me_ref, tp, store)
    out_ref[...] = product_of(x_refs, matrix_ref, rows_ref)


def gate_rows(me, rows, parts):
    tp = len(parts)
    fs, height, cols = parts[0].shape
    matrix = (fs * height, tp * cols)
    out = (tp * rows[0].shape[0], tp * cols)
    return pl.pallas_call(
        functools.partial(gate_kernel, fs, tp),
        grid_spec=pltpu.PrefetchScalarGridSpec(
            num_scalar_prefetch=1,
            grid=(1,),
            in_specs=[whole(rows[0].shape)] * tp + [whole(parts[0].shape)] * tp,
            out_specs=[whole(matrix), whole(out)],
            scratch_shapes=[pltpu.VMEM((out[0], matrix[0]), bf16)],
        ),
        out_shape=[jax.ShapeDtypeStruct(matrix, bf16), jax.ShapeDtypeStruct(out, f32)],
        compiler_params=grant(24),
        cost_estimate=cost(2 * out[0] * matrix[0] * matrix[1], 4 * matrix[0] * matrix[1]),
    )(me, *rows, *parts)


def assemble(me_ref, parts, matrix_ref):
    fs, rows = len(parts), parts[0].shape[0]
    if fs == 1:
        matrix_ref[...] = parts[0][...]
        return
    for r in range(fs):
        origin = lax.rem(me_ref[0] - r + fs, fs)
        matrix_ref[pl.ds(pl.multiple_of(origin * rows, rows), rows), :] = parts[r][...]


def up_kernel(tp, me_ref, *refs):
    x_refs, parts, refs = refs[:tp], refs[tp:-4], refs[-4:]
    gate_ref, matrix_ref, out_ref, rows_ref = refs
    assemble(me_ref, parts, matrix_ref)
    up = product_of(x_refs, matrix_ref, rows_ref)
    gate = gate_ref[...]
    out_ref[...] = (gate / (1.0 + jnp.exp(-gate)) * up).astype(bf16)


def up_rows(me, rows, parts, gate):
    tp = len(rows)
    matrix = (len(parts) * parts[0].shape[0], parts[0].shape[1])
    return pl.pallas_call(
        functools.partial(up_kernel, tp),
        grid_spec=pltpu.PrefetchScalarGridSpec(
            num_scalar_prefetch=1,
            grid=(1,),
            in_specs=[whole(rows[0].shape)] * tp
            + [whole(part.shape) for part in parts]
            + [whole(gate.shape)],
            out_specs=[whole(matrix), whole(gate.shape)],
            scratch_shapes=[pltpu.VMEM((gate.shape[0], matrix[0]), bf16)],
        ),
        out_shape=[jax.ShapeDtypeStruct(matrix, bf16), jax.ShapeDtypeStruct(gate.shape, bf16)],
        compiler_params=grant(24),
        cost_estimate=cost(2 * gate.size * matrix[0], 4 * matrix[0] * matrix[1]),
    )(me, *rows, *parts, gate)


def down_kernel(count_parts, tp, low, aliased, me_ref, hidden_ref, *refs):
    w_refs, refs = refs[:tp], refs[tp:]
    parts, refs = refs[:count_parts], refs[count_parts:]
    if aliased:
        refs = refs[1:]
    matrix_ref, same_ref, other_ref, block, done = refs
    assemble(me_ref, parts, block)
    copy = pltpu.make_async_copy(block, matrix_ref.at[:, pl.ds(low, block.shape[1])], done)
    copy.start()
    product = jnp.dot(hidden_ref[...], block[...], preferred_element_type=f32)
    product = product.astype(bf16).astype(f32)
    count = w_refs[0].shape[0]
    lane = lax.broadcasted_iota(jnp.int32, (count, lanes), 1)
    mine = me_ref[1]
    chosen = (lane == mine) | (lane == mine + tp) | (lane == mine + 2 * tp)
    for q in range(tp):
        weight = jnp.sum(
            jnp.where(chosen, w_refs[q][...].astype(f32), 0.0), axis=1, keepdims=True
        )
        out_ref, at = (same_ref, q) if q < tp // 2 else (other_ref, q - tp // 2)
        out_ref[at * count : (at + 1) * count] = (
            product[q * count : (q + 1) * count] * weight
        ).astype(bf16)
    copy.wait()


def down_rows(me, hidden, rows, parts, low, width, prior):
    tp = len(rows)
    count = rows[0].shape[0]
    depth = hidden.shape[1]
    size = parts[0].shape[1]
    weight_block = width // lanes
    in_specs = [whole(hidden.shape)]
    in_specs += [pl.BlockSpec((count, lanes), lambda k, m: (0, weight_block))] * tp
    in_specs += [whole(part.shape) for part in parts]
    args = [hidden, *rows, *parts]
    aliases = {}
    if prior is not None:
        in_specs.append(pl.BlockSpec(memory_space=pl.ANY))
        args.append(prior)
        aliases = {len(args): 0}
    outs = pl.pallas_call(
        functools.partial(down_kernel, len(parts), tp, low, prior is not None),
        grid_spec=pltpu.PrefetchScalarGridSpec(
            num_scalar_prefetch=1,
            grid=(1,),
            in_specs=in_specs,
            out_specs=[pl.BlockSpec(memory_space=pl.ANY)] + [whole((tp // 2 * count, size))] * 2,
            scratch_shapes=[pltpu.VMEM((depth, size), bf16), pltpu.SemaphoreType.DMA],
        ),
        out_shape=[jax.ShapeDtypeStruct((depth, width), bf16)]
        + [jax.ShapeDtypeStruct((tp // 2 * count, size), bf16)] * 2,
        input_output_aliases=aliases,
        compiler_params=grant(16),
        cost_estimate=cost(2 * tp * count * depth * size, 4 * depth * size),
    )(me, *args)
    return outs


def final_kernel(fs, tp, ids_ref, back_ref, out_ref):
    onehot = slot_onehot(group_of(ids_ref[0:1, :], fs, tp), fs)
    out_ref[...] = jnp.dot(onehot, back_ref[...], preferred_element_type=f32).astype(bf16)


def shards(tokens, norm_gain, gate_proj, up_proj, down_proj, expert_ids, route_weight):
    fs = lax.axis_size("fs")
    tp = lax.axis_size("tp")
    me = jnp.stack([lax.axis_index("fs"), lax.axis_index("tp")]).astype(jnp.int32)
    count, width = tokens.shape
    cuts = cuts_of(width)

    def rotate(parts, axis, distances=None):
        n = len(parts)
        out = list(parts)
        for r in distances or far_first(n):
            out[r] = lax.ppermute(parts[r], axis, [(k, (k + r) % n) for k in range(n)])
        return out

    def swap_fs(value):
        out = lax.all_to_all(value, "fs", 0, 0, tiled=True)
        return out.reshape(-1, out.shape[2])

    def swap_core(value):
        return lax.ppermute(value, "tp", [(j, j ^ 1) for j in range(tp)])

    def by_expert(matrix):
        return matrix.reshape((fs, tp) + matrix.shape[1:])

    ids, weights = expert_ids.T, route_weight.T
    scale = norm_gain[None, :]

    sent = pl.pallas_call(
        functools.partial(prep_kernel, fs, tp),
        out_shape=jax.ShapeDtypeStruct((count, width + lanes), bf16),
        cost_estimate=cost(2 * count * count * width, 4 * count * width),
    )(tokens, ids, weights)
    landed = swap_fs(sent.reshape(fs, count // fs, -1))
    gate_parts = [None] * fs
    early, late = far_first(fs)[:3], far_first(fs)[3:]

    def cut_gate(distances, params):
        cut = cast_along(me, by_expert(gate_proj), scale, 0, distances, params)
        for r, part in zip(distances, cut):
            gate_parts[r] = part
        gate_parts[:] = rotate(gate_parts, "fs", distances=[r for r in distances if r > 0])

    cut_gate(early, None)
    up_parts = cast_along(me, by_expert(up_proj), scale, 1, range(tp), grant(16))
    up_parts = rotate(up_parts, "tp")
    cut_gate(late + [0], grant(16))
    down_parts = cast_along(me, by_expert(down_proj), None, 1, range(tp), grant(16))
    down_parts = rotate(down_parts, "tp")
    rows = [landed] + [
        lax.ppermute(landed, "tp", [(k, (k + step) % tp) for k in range(tp)])
        for step in range(2, tp, 2)
    ]
    rows += [swap_core(part) for part in rows]
    (up_parts,) = merge(me, up_parts, [(0, tp * up_parts[0].shape[2])])
    up_parts = rotate(up_parts, "fs")
    gate_parts = regroup(me, gate_parts)
    gate_parts = rotate(gate_parts, "tp")
    down_parts = merge(me, down_parts, cuts)
    new_gate, gate = gate_rows(me, rows, gate_parts)
    down_parts[0] = rotate(down_parts[0], "fs")
    down_parts[1] = rotate(down_parts[1], "fs")
    new_up, hidden = up_rows(me, rows, up_parts, gate)
    new_down = None
    sums = []
    for k, (low, _) in enumerate(cuts):
        new_down, mine, other = down_rows(
            me, hidden, rows, down_parts[k], low, width, new_down
        )
        other = swap_core(other)
        terms = fold(count, mine, other)
        terms = [terms[0]] + [
            lax.ppermute(term, "tp", [(j, (j - step) % tp) for j in range(tp)])
            for term, step in zip(terms[1:], range(2, tp, 2))
        ]
        sums.append(terms)
    summed = add(fs, sums)
    back = swap_fs(summed)
    mixed = pl.pallas_call(
        functools.partial(final_kernel, fs, tp),
        out_shape=jax.ShapeDtypeStruct((count, width), bf16),
        compiler_params=grant(16),
        cost_estimate=cost(2 * count * count * width, 4 * count * width),
    )(ids, back)
    return (mixed, new_gate[None], new_up[None], new_down[None])


def solution(mesh):
    in_specs = (
        P(("fs", "tp"), None),
        P("fs"),
        P(None, "fs", "tp"),
        P(None, "fs", "tp"),
        P(None, "fs", "tp"),
        P(("fs", "tp"), None),
        P(("fs", "tp"), None),
    )
    out_specs = (
        P(("fs", "tp"), None),
        P(("fs", "tp"), None, None),
        P(("fs", "tp"), None, None),
        P(("fs", "tp"), None, None),
    )

    return jax.shard_map(shards, mesh=mesh, in_specs=in_specs, out_specs=out_specs, check_vma=False)
```
